32 devices in a mesh: grp: 2 (over y), ep: 4 (over z), tp: 4 (over x, core).
Axes of the slice: x: 2, y: 2, z: 4, core: 2. Of those that a mesh axis runs over, the one named last changes fastest.
Arguments:
- queries: bfloat16 [1024, 2048], P(('grp', 'ep'), 'tp'), parts along dimension 0, may hold values from -6 to 6
- keys: bfloat16 [1024, 2048], P(('grp', 'ep'), 'tp'), parts along dimension 0, may hold values from -6 to 6
- values: bfloat16 [1024, 2048], P(('grp', 'ep'), 'tp'), parts along dimension 0, may hold values from -6 to 6
- stop_bias: bfloat16 [1024, 32], P(('grp', 'ep'), 'tp'), parts along dimension 0, may hold values from -20 to 0
- out_weight: bfloat16 [2048, 2048], P('tp'), may hold values from -0.125 to 0.125
- mix_gain: float32 [2048], replicated, may hold values from 0.1 to 1.9
- moe_input: bfloat16 [4096, 2048], P(('grp', 'ep', 'tp')), parts along dimension 0, may hold values from -6 to 6
- ffn_gain: float32 [2048], replicated, may hold values from 0.1 to 1.9
- expert_ids: int32 [4096, 2], P(('grp', 'ep', 'tp')), parts along dimension 0, may hold values from 0 to 3, all different within a row; in each aligned block of 128 rows (0 to 127, 128 to 255, ...) at most 96 rows name the same one
- expert_scores: float32 [4096, 2], P(('grp', 'ep', 'tp')), parts along dimension 0, may hold values from 0.05 to 1
- gate_weight: bfloat16 [4, 2048, 1024], P('ep', None, 'tp'), may hold values from -0.125 to 0.125
- up_weight: bfloat16 [4, 2048, 1024], P('ep', None, 'tp'), may hold values from -0.125 to 0.125
- down_weight: bfloat16 [4, 1024, 2048], P('ep', 'tp'), may hold values from -0.1875 to 0.1875
Outputs:
- mixed: bfloat16 [1024, 2048], P(('grp', 'ep', 'tp')), parts along dimension 0
- experts_mixed: bfloat16 [4096, 2048], P(('grp', 'ep', 'tp')), parts along dimension 0
The draws below stay inside these ranges and needn't reach their ends.
There are 2 independent parts, one for each index of `grp`. The reference program is written for one: setup_inputs(seed, part) draws one part's arguments, and reference() takes and returns one part's arrays. A program takes and returns all parts, laid end to end along the dimension named above; an argument that names none is the same for every part. Nothing has to cross between parts.
Inputs may be any that keep to these rules, and one draw needn't show every extreme that they name: `expert_ids`: each token names 2 different experts. Among the 128 tokens of one device, no expert is named by more than 96 tokens, and in some device's tokens some expert is named by exactly 96.
All inputs are finite; a program needn't handle non-finite values.
Results may differ from the reference program's by a relative error of at most 0.012.
Values may be sent and summed in bfloat16 or wider, within the bound.
A program may use at most 128 MiB of HBM per device.

```python
import math
import jax
import jax.numpy as jnp
import numpy as np
from jax import lax

D = 2048
HEADS = 32
HEAD = 64
FF = 1024
TOP_K = 2
SEQ_DEV = 128
TOK_DEV = 128
CONTEXT_LENGTH = 512
TOKENS = 2048
EXPERTS = 4
CAP = 96
N_EP = 4
N_TP = 4


def draw_stop_bias(key, part):
    streams = jax.random.split(key, 7)
    fast = jax.random.uniform(streams[0], (HEADS,)) < 0.5
    slow_rate = jax.random.uniform(streams[1], (HEADS,), minval=0.1, maxval=0.4) / CONTEXT_LENGTH
    fast_rate = jax.random.uniform(streams[2], (HEADS,), minval=1.0 / 150.0, maxval=1.0 / 60.0)
    starting_level = jnp.log(jnp.where(fast, fast_rate, slow_rate))
    displacement_delta = jax.random.uniform(streams[3], (CONTEXT_LENGTH // SEQ_DEV, 1), minval=-0.7, maxval=0.7)
    displacement_delta = jnp.repeat(displacement_delta, SEQ_DEV, axis=0)
    approximate_guess = jax.random.uniform(streams[4], (CONTEXT_LENGTH, HEADS), minval=-2.0, maxval=2.0)
    location_number = jax.random.randint(streams[5], (4,), 0, CONTEXT_LENGTH)
    spike_height = jnp.any(jnp.arange(CONTEXT_LENGTH)[:, None] == location_number[None, :], axis=1)
    intensity_multiplier = jax.random.uniform(streams[6], (CONTEXT_LENGTH, HEADS), minval=0.25, maxval=0.4)
    closing_answer = jnp.where(spike_height[:, None], jnp.log(intensity_multiplier / (1.0 - intensity_multiplier)), starting_level[None, :] + displacement_delta + approximate_guess)
    return closing_answer.astype(jnp.bfloat16)


def level_of(key, extent, cuts, low, largest):
    def one(position, blocks):
        heights = jax.random.uniform(jax.random.fold_in(jax.random.fold_in(key, 6), position), (blocks,), jnp.float32, low / len(cuts), largest / len(cuts))
        return jnp.repeat(jnp.exp(heights), extent[position] // blocks).reshape((-1,) + (1,) * (len(extent) - position - 1))

    loudness = one(*cuts[0])
    for cut in cuts[1:]:
        loudness = loudness * one(*cut)
    return loudness


def routed_block(stream_key, own, number, rows, amount, top, limit, slope):
    sequence = jax.random.permutation(stream_key, amount)
    heavy_load, usual = shares(amount, rows * top, limit, slope, True), shares(amount, rows * top, limit, slope, False)
    places = jnp.arange(amount)

    def named(tallies, turn):
        used = int((tallies > 0).sum())
        fixed = max(1, used // 4)
        shifted = fixed + (places - fixed + turn * (used - fixed)) % max(1, amount - fixed)
        return jnp.zeros((amount,), jnp.int32).at[sequence[jnp.where(places < fixed, places, shifted)]].set(jnp.asarray(tallies, jnp.int32))

    tallies = jnp.where(number % 4 == 0, named(heavy_load, number // 4), named(usual, number - number // 4 - 1))
    mixed = jax.random.permutation(jax.random.fold_in(own, 3), amount)
    giver, sink = mixed[0:amount // 2 * 2:2], mixed[1:amount // 2 * 2:2]
    margin = jnp.minimum(tallies[giver] - 1, limit - tallies[sink]) // 2
    margin = jnp.where((giver == sequence[0]) | (sink == sequence[0]) | (tallies[sink] == 0), 0, jnp.maximum(margin, 0))
    shifted = jax.random.randint(jax.random.fold_in(own, 4), (amount // 2,), 0, 1 << 20) % (margin + 1)
    tallies = tallies.at[giver].add(-shifted).at[sink].add(shifted)
    members = jnp.searchsorted(jnp.cumsum(tallies), jnp.arange(rows * top), side="right").astype(jnp.int32)
    table = members.reshape(top, rows).T
    table = table[jax.random.permutation(jax.random.fold_in(own, 1), rows)]
    turn = jax.random.randint(jax.random.fold_in(own, 2), (rows, 1), 0, top)
    return jnp.take_along_axis(table, (jnp.arange(top)[None, :] + turn) % top, axis=1)


def shares(number_of, total, bound, skew, full):
    loads = [(1 << 20) // math.isqrt(standing ** skew) + 1 for standing in range(1, number_of + 1)]
    largest = bound if full else min(bound, max(-(-total // number_of), total * loads[0] // sum(loads)))
    least = 1 if total - largest >= number_of - 1 else 0
    counts, spare = [largest] + [least] * (number_of - 1), total - largest - least * (number_of - 1)
    while spare > 0:
        candidates = [i for i in range(1, number_of) if counts[i] < largest] or [i for i in range(1, number_of) if counts[i] < bound]
        mass, remaining = sum([loads[i] for i in candidates]), spare
        for i in candidates:
            addition = min(bound - counts[i], max(1, remaining * loads[i] // mass), spare)
            counts[i] = counts[i] + addition
            spare = spare - addition
    return np.array(counts)


def scatter_about(own_key, shape, scale, bound, cuts=(), held_as=jnp.bfloat16):
    values = jax.random.normal(own_key, shape, jnp.float32) * scale
    if len(cuts) > 0:
        values = level_of(own_key, shape, cuts, -0.22, 0.18) * values
    return jnp.clip(values, min=-bound, max=bound).astype(held_as)


def setup_inputs(seed: int = 0, part: int = 0) -> dict:
    key_of = jax.random.split(jax.random.key(seed), 14)
    own_keys = jax.random.split(jax.random.fold_in(key_of[13], part), 14)
    queries = scatter_about(own_keys[0], (CONTEXT_LENGTH, HEADS * HEAD), 1.0, 6.0, ((0, 4), (1, 4)))
    keys = scatter_about(own_keys[1], (CONTEXT_LENGTH, HEADS * HEAD), 1.0, 6.0, ((0, 4), (1, 4)))
    values = scatter_about(own_keys[2], (CONTEXT_LENGTH, HEADS * HEAD), 1.0, 6.0, ((0, 4), (1, 4)))
    stop_bias = draw_stop_bias(jax.random.fold_in(jax.random.fold_in(key_of[13], part), 71), part)
    out_weight = scatter_about(key_of[4], (HEADS * HEAD, D), (HEADS * HEAD) ** -0.5, 0.125, ((0, 4),))
    mix_gain = jnp.clip(1.0 + 0.18 * jax.random.normal(key_of[5], (D,), jnp.float32), 0.1, 1.9)
    moe_input = scatter_about(own_keys[6], (TOKENS, D), 1.0, 6.0, ((0, 16),))
    ffn_gain = jnp.clip(1.0 + 0.18 * jax.random.normal(key_of[7], (D,), jnp.float32), 0.1, 1.9)
    expert_ids_keys = jax.random.split(jax.random.fold_in(own_keys[8], 1), TOKENS // TOK_DEV)
    expert_ids_turns = jax.random.permutation(jax.random.fold_in(own_keys[8], 3), TOKENS // TOK_DEV)
    expert_ids = jax.vmap(lambda own, number: routed_block(jax.random.fold_in(own_keys[8], 2), own, number, TOK_DEV, EXPERTS, TOP_K, CAP, 2))(expert_ids_keys, expert_ids_turns).reshape((TOKENS, TOP_K))
    expert_scores = jnp.clip(jnp.exp(math.log(1.0) - 2.9957323 * jax.random.uniform(own_keys[9], (TOKENS, TOP_K), jnp.float32) ** level_of(own_keys[9], (TOKENS, TOP_K), ((0, 16),), -0.2, 0.2)), 0.05, 1.0)
    gate_weight = scatter_about(key_of[10], (EXPERTS, D, FF), D ** -0.5, 0.125, ((0, 4), (2, 4)))
    up_weight = scatter_about(key_of[11], (EXPERTS, D, FF), D ** -0.5, 0.125, ((0, 4), (2, 4)))
    down_weight = scatter_about(key_of[12], (EXPERTS, FF, D), FF ** -0.5, 0.1875, ((0, 4), (1, 4)))
    return dict(queries=queries, keys=keys, values=values, stop_bias=stop_bias, out_weight=out_weight, mix_gain=mix_gain, moe_input=moe_input, ffn_gain=ffn_gain, expert_ids=expert_ids, expert_scores=expert_scores, gate_weight=gate_weight, up_weight=up_weight, down_weight=down_weight)


def norm_rows(values, gain):
    values = values.astype(jnp.float32)
    scale = lax.rsqrt(lax.optimization_barrier(jnp.mean(values * values, axis=-1, keepdims=True)) + 1e-06)
    return values * scale * gain

def settle(term):
    return lax.optimization_barrier(term.astype(jnp.bfloat16)).astype(jnp.float32)

def stick_head(inputs):
    query, key, value, bias = inputs
    length = query.shape[0]
    count = length // SEQ_DEV
    scores = jnp.dot(query, key.T, preferred_element_type=jnp.float32) * HEAD ** (-0.5)
    scores = scores + bias.astype(jnp.float32)[None, :]
    place = jnp.arange(length)
    past = place[None, :] < place[:, None]
    rest = jnp.where(past, jax.nn.log_sigmoid(-scores), 0.0)
    rest_blocks = rest.reshape(length, count, SEQ_DEV)
    later = lax.cumsum(rest_blocks, axis=2, reverse=True)
    within = (later - rest_blocks).reshape(length, length)
    totals = later[:, :, 0]
    local = jnp.where(past, jnp.exp(jax.nn.log_sigmoid(scores) + within), 0.0).astype(jnp.bfloat16)
    parts = jnp.einsum('tbs,bsd->tbd', local.reshape(length, count, SEQ_DEV).astype(jnp.float32), value.reshape(count, SEQ_DEV, HEAD).astype(jnp.float32), precision=lax.Precision.HIGHEST)
    carried = lax.cumsum(totals, axis=1, reverse=True) - totals
    return lax.optimization_barrier(jnp.sum(jnp.exp(carried)[:, :, None] * parts, axis=1))

def reference(queries, keys, values, stop_bias, out_weight, mix_gain, moe_input, ffn_gain, expert_ids, expert_scores, gate_weight, up_weight, down_weight):
    length = queries.shape[0]

    def by_head(array):
        return array.reshape(length, HEADS, HEAD).transpose(1, 0, 2)
    attended = lax.map(stick_head, (by_head(queries), by_head(keys), by_head(values), stop_bias.T))
    attended = attended.transpose(1, 0, 2).reshape(length, HEADS * HEAD).astype(jnp.bfloat16)
    group = HEADS * HEAD // N_TP
    projected = jnp.zeros((length, D), jnp.float32)
    for quarter in range(N_TP):
        term = jnp.dot(attended[:, quarter * group:(quarter + 1) * group], out_weight[quarter * group:(quarter + 1) * group], preferred_element_type=jnp.float32)
        projected = projected + settle(term)
    mixed = norm_rows(projected, mix_gain).astype(jnp.bfloat16)
    normed = norm_rows(moe_input, ffn_gain).astype(jnp.bfloat16)
    weights = expert_scores / lax.optimization_barrier(jnp.sum(expert_scores, axis=1, keepdims=True))
    load = N_EP * N_TP * CAP
    share = FF // N_TP

    def one_expert(total, expert):
        named = expert_ids == expert
        present = jnp.any(named, axis=1)
        weight = lax.optimization_barrier(jnp.sum(jnp.where(named, weights, 0.0), axis=1))
        chosen = jnp.nonzero(present, size=load, fill_value=0)[0].astype(jnp.int32)
        valid = jnp.arange(load) < jnp.sum(present.astype(jnp.int32))
        rows = normed[chosen]
        gate = jnp.dot(rows, gate_weight[expert], preferred_element_type=jnp.float32)
        upward = jnp.dot(rows, up_weight[expert], preferred_element_type=jnp.float32)
        hidden = (jax.nn.silu(gate) * upward).astype(jnp.bfloat16)
        lowering = down_weight[expert]
        summed = jnp.zeros((load, D), jnp.float32)
        for quarter in range(N_TP):
            term = jnp.dot(hidden[:, quarter * share:(quarter + 1) * share], lowering[quarter * share:(quarter + 1) * share], preferred_element_type=jnp.float32)
            summed = summed + settle(term)
        output = settle(summed)
        contribution = jnp.where(valid[:, None], weight[chosen][:, None] * output, 0.0)
        return (total.at[chosen].add(contribution), None)
    total, _ = lax.scan(one_expert, jnp.zeros((TOKENS, D), jnp.float32), jnp.arange(EXPERTS, dtype=jnp.int32))
    return (mixed, total.astype(jnp.bfloat16))
```

```python
import functools

import jax
import jax.numpy as jnp
from jax import lax
from jax.experimental import pallas as pl
from jax.experimental.pallas import tpu as pltpu
from jax.sharding import PartitionSpec as P

MESH = pl.DeviceIdType.MESH
F32 = jnp.float32
BF16 = jnp.bfloat16


def norm_rows(values, gain):
    values = values.astype(jnp.float32)
    scale = lax.rsqrt(jnp.mean(values * values, axis=-1, keepdims=True) + 1e-06)
    return values * scale * gain


def break_terms(query_heads, query_place, key_block, bias_block, first):
    span = key_block.shape[0]
    heads = query_heads.shape[1]
    key_heads = key_block.reshape(span, heads, -1)
    scores = jnp.einsum("qhd,khd->hqk", query_heads, key_heads, preferred_element_type=jnp.float32)
    scores = scores * query_heads.shape[2] ** (-0.5) + bias_block.astype(jnp.float32).T[:, None, :]
    key_place = first + jnp.arange(span)
    past = (key_place[None, :] < query_place[:, None])[None]
    rest = jnp.where(past, jax.nn.log_sigmoid(-scores), 0.0)
    later = lax.cumsum(rest, axis=2, reverse=True)
    return (scores, past, rest, later)


def block_part(scores, past, rest, later, value_block, heads):
    within = later - rest
    local = jnp.where(past, jnp.exp(jax.nn.log_sigmoid(scores) + within), 0.0).astype(jnp.bfloat16)
    span = value_block.shape[0]
    value_heads = value_block.reshape(span, heads, -1)
    part = jnp.einsum("hqk,khd->qhd", local, value_heads, preferred_element_type=jnp.float32)
    return part.reshape(part.shape[0], -1)


def keep(state):
    return state


def dispatch_plan(normed, expert_ids, experts, capacity):
    rows, top = expert_ids.shape
    flat_ids = expert_ids.reshape(rows * top)
    onehot = (flat_ids[:, None] == jnp.arange(experts)[None, :]).astype(jnp.int32)
    earlier = jnp.cumsum(onehot, axis=0) - onehot
    place = jnp.sum(earlier * onehot, axis=1)
    target = flat_ids * capacity + place
    source = (
        jnp.zeros((experts * capacity,), jnp.int32)
        .at[target]
        .set(jnp.arange(rows * top, dtype=jnp.int32) // top + 1)
    )
    padded = jnp.concatenate([jnp.zeros((1, normed.shape[1]), normed.dtype), normed], axis=0)
    return (padded[source].reshape(experts, capacity, normed.shape[1]), target)


def expert_hidden(piece, gate_weight, up_weight):
    flat = piece.reshape(-1, piece.shape[-1])
    gate = jnp.dot(flat, gate_weight[0], preferred_element_type=jnp.float32)
    upward = jnp.dot(flat, up_weight[0], preferred_element_type=jnp.float32)
    hidden = (jax.nn.silu(gate) * upward).astype(jnp.bfloat16)
    return hidden.reshape(piece.shape[0], piece.shape[1], -1)


def send_back(summed):
    return lax.all_to_all(
        summed.astype(jnp.bfloat16), "ep", split_axis=0, concat_axis=0, tiled=True
    )


def return_rows(hidden_all, down_weight, sources):
    flat = hidden_all.reshape(-1, hidden_all.shape[2])
    product = jnp.dot(flat, down_weight[0], preferred_element_type=jnp.float32)
    return send_back(
        lax.psum_scatter(
            product.reshape(sources * lax.axis_size("tp"), hidden_all.shape[1], -1).astype(
                jnp.bfloat16
            ),
            "tp",
            scatter_dimension=0,
            tiled=True,
        ).astype(jnp.float32)
    )


def per_device(
    queries,
    keys,
    values,
    stop_bias,
    out_weight,
    mix_gain,
    moe_input,
    ffn_gain,
    expert_ids,
    expert_scores,
    gate_weight,
    up_weight,
    down_weight,
):
    span = queries.shape[0]
    heads = stop_bias.shape[1]
    width_heads = queries.shape[1]
    blocks = lax.axis_size("ep")
    own_first = lax.axis_index("ep") * span
    query_heads = queries.reshape(span, heads, -1)
    query_place = own_first + jnp.arange(span)

    def piece_rows(piece, index):
        return tuple((lax.dynamic_slice_in_dim(member, index * span, span, 0) for member in piece))

    start_state = (
        jnp.zeros((blocks, heads, span), jnp.float32),
        jnp.zeros((blocks, span, width_heads), jnp.float32),
    )
    piece = (
        lax.all_gather(keys, "ep", axis=0, tiled=True),
        lax.all_gather(values, "ep", axis=0, tiled=True),
        lax.all_gather(stop_bias, "ep", axis=0, tiled=True),
    )

    def one_block(index, state):
        key_block, value_block, bias_block = piece_rows(piece, index)
        first = index * span

        def compute(inner_state):
            totals, parts = inner_state
            scores, past, rest, later = break_terms(
                query_heads, query_place, key_block, bias_block, first
            )
            part = block_part(scores, past, rest, later, value_block, heads)
            number = first // span
            totals = lax.dynamic_update_index_in_dim(totals, later[:, :, 0], number, 0)
            parts = lax.dynamic_update_index_in_dim(parts, part, number, 0)
            return (totals, parts)

        return lax.cond(first <= own_first, compute, keep, state)

    totals, parts = lax.fori_loop(0, piece[0].shape[0] // span, one_block, start_state)
    carried = lax.cumsum(totals, axis=0, reverse=True) - totals
    factor = jnp.exp(carried).transpose(0, 2, 1)[:, :, :, None]
    attended = jnp.sum(factor * parts.reshape(blocks, span, heads, -1), axis=0).reshape(
        span, width_heads
    )
    attended = attended.astype(jnp.bfloat16)
    projected = lax.psum_scatter(
        jnp.dot(attended, out_weight, preferred_element_type=jnp.float32).astype(jnp.bfloat16),
        "tp",
        scatter_dimension=0,
        tiled=True,
    ).astype(jnp.float32)
    mixed = norm_rows(projected, mix_gain).astype(jnp.bfloat16)
    normed = norm_rows(moe_input, ffn_gain).astype(jnp.bfloat16)
    rows, top = expert_ids.shape
    experts = lax.axis_size("ep")
    capacity = 3 * rows * top // (2 * experts)
    weights = expert_scores / jnp.sum(expert_scores, axis=1, keepdims=True)
    outbound, target = dispatch_plan(normed, expert_ids, experts, capacity)
    arrived = lax.all_to_all(outbound, "ep", split_axis=0, concat_axis=0, tiled=True)
    hidden_all = expert_hidden(
        lax.all_gather(arrived, "tp", axis=0, tiled=True), gate_weight, up_weight
    )
    returned = return_rows(hidden_all, down_weight, arrived.shape[0])
    picked = returned.reshape(experts * capacity, -1)[target].reshape(rows, top, -1)
    experts_mixed = jnp.sum(picked.astype(jnp.float32) * weights[:, :, None], axis=1).astype(
        jnp.bfloat16
    )
    return (mixed, experts_mixed)


def layer_kernel(
    ep,
    capacity,
    head,
    q_ref,
    k_ref,
    v_ref,
    bias_ref,
    ow_ref,
    mix_gain_ref,
    x_ref,
    ffn_gain_ref,
    ids_ref,
    scores_ref,
    g_ref,
    u_ref,
    d_ref,
    mixed_ref,
    out_ref,
    x_own,
    gain_own,
    mix_own,
    ids_own,
    scores_own,
    qkv_all,
    bias_all,
    bias_rows,
    att_send,
    att_all,
    proj,
    proj_in,
    ow,
    meta,
    meta_in,
    normed_ref,
    dense_in,
    sel,
    sel_back,
    gate_cols,
    outbound,
    relay_out,
    rows_in,
    hid,
    acc,
    back_out,
    back_in,
    outer_out,
    outer_in,
    dense_out,
    dense_back,
    g_all,
    u_all,
    d_all,
    load_sem,
    own_sem,
    ow_sem,
    pack_send,
    pack_recv,
    bias_send,
    bias_recv,
    row_send,
    row_recv,
    meta_send,
    meta_recv,
    dense_send,
    dense_recv,
    relay_send,
    relay_recv,
    att_ssem,
    att_rsem,
    back_ssem,
    back_rsem,
    outer_send,
    outer_recv,
    home_send,
    home_recv,
    proj_ssem,
    proj_rsem,
    near_send,
    near_recv,
    x_send,
    x_recv,
    y_send,
    y_recv,
    cross_send,
    cross_wide,
    cross_down,
):
    me = lax.axis_index("ep")
    tp = lax.axis_index("tp")
    grp = lax.axis_index("grp")
    chip, core = tp // 2, tp % 2
    mates = [None, chip * 2 + (1 - core), (1 - chip) * 2 + core, (1 - chip) * 2 + (1 - core)]
    span = q_ref.shape[0]
    width = qkv_all.shape[3]
    heads = width // head
    tokens, deep = x_ref.shape
    top = ids_ref.shape[0]
    parts = dense_recv.shape[1]
    fine = home_recv.shape[0]
    wide_cuts = 2 * g_ref.shape[1]

    half = me // 2
    is_inner = lax.rem(me + 1, ep) // 2
    inner = is_inner == 1
    outside = is_inner == 0
    side = me + 1 - 2 * (me % 2)
    far = (3 * (1 - half), 2 - half)

    loads = [
        pltpu.make_async_copy(s, t, load_sem.at[n])
        for n, (s, t) in enumerate(
            (
                (x_ref, x_own),
                (ids_ref, ids_own),
                (scores_ref, scores_own),
                (ffn_gain_ref, gain_own),
                (g_ref, g_all.at[0]),
                (u_ref, u_all.at[0]),
                (d_ref, d_all.at[0]),
                (mix_gain_ref, mix_own),
                (bias_ref, bias_all.at[me]),
            )
        )
    ]
    own = pl.ds(pl.multiple_of(me * width, width), width)
    mine = [
        pltpu.make_async_copy(r.at[:, own], qkv_all.at[me, n], own_sem.at[n])
        for n, r in enumerate((q_ref, k_ref, v_ref))
    ]
    ow_copy = pltpu.make_async_copy(ow_ref, ow, ow_sem)
    for copy in loads:
        copy.start()

    barrier = pltpu.get_barrier_semaphore()
    peers = [{"ep": lax.rem(me + r, ep)} for r in range(1, ep)]
    peers += [{"tp": mates[m]} for m in (1, 2, 3)] + [{"grp": 1 - grp}]
    for peer in peers:
        pl.semaphore_signal(barrier, inc=1, device_id=peer, device_id_type=MESH)
    for copy in mine:
        copy.start()
    ow_copy.start()

    def send(src, dst, ssem, rsem, peer):
        return pltpu.make_async_remote_copy(
            src_ref=src,
            dst_ref=dst,
            send_sem=ssem,
            recv_sem=rsem,
            device_id=peer,
            device_id_type=MESH,
        )

    mate = {"tp": mates[1]}

    def arrived(ref, sem):
        send(ref, ref, sem, sem, mate).wait_recv()

    def drained(ref, sem):
        send(ref, ref, sem, sem, mate).wait_send()

    def cols_of(c, n=parts):
        return slice(c * (deep // n), (c + 1) * (deep // n))

    def piece_of(n, s, g):
        if n < wide_cuts:
            return (g_all, u_all)[n % 2].at[s, g, n // 2]
        return d_all.at[s, g, :, cols_of(n - wide_cuts, fine)]

    def kind_of(n):
        return n % 2 if n < wide_cuts else 2

    chunks = wide_cuts + fine

    for n in range(4):
        loads[n].wait()
    gates = scores_own[...]
    gates = gates / jnp.sum(gates, axis=0, keepdims=True)
    meta[...] = jnp.zeros_like(meta)
    meta[0:top] = ids_own[...].astype(F32)
    meta[top : 2 * top] = gates
    values = x_own[...].astype(F32)
    scale = lax.rsqrt(jnp.mean(values * values, axis=-1, keepdims=True) + 1e-06)
    normed_ref[...] = (values * scale * gain_own[...]).astype(BF16)

    pl.semaphore_wait(barrier, len(peers))

    def over_x(n):
        return send(
            piece_of(n, 0, grp),
            piece_of(n, 2, grp),
            x_send.at[kind_of(n)],
            x_recv.at[n],
            {"tp": mates[2]},
        )

    loads[4].wait()
    over_x(0).start()
    send(meta, meta_in.at[is_inner], meta_send, meta_recv.at[is_inner], {"ep": far[1]}).start()

    def dense_of(slot, c):
        return send(
            normed_ref.at[:, cols_of(c)],
            dense_in.at[slot, :, cols_of(c)],
            dense_send,
            dense_recv.at[slot, c],
            {"ep": far[1]},
        )

    for c in range(parts):
        dense_of(is_inner, c).start()
    loads[5].wait()
    for n in range(1, wide_cuts):
        over_x(n).start()
    loads[6].wait()
    for n in range(wide_cuts, chunks):
        over_x(n).start()
    nears = [
        send(r.at[0], r.at[1], near_send.at[n], near_recv.at[n], mate)
        for n, r in enumerate((g_all, u_all, d_all))
    ]
    for copy in nears:
        copy.start()

    square = (tokens, tokens)
    lane = lax.broadcasted_iota(jnp.int32, square, 1)
    sub = lax.broadcasted_iota(jnp.int32, square, 0)
    earlier = (sub < lane).astype(BF16)
    slots = lax.broadcasted_iota(jnp.int32, (capacity, tokens), 0).astype(F32)

    def route(table, at):
        named = jnp.zeros(square, F32)
        gate = jnp.zeros(square, F32)
        for n, e in enumerate((me, side)):
            place_of = e.astype(F32)
            for k in range(top):
                hit = table[k : k + 1, :] == place_of
                here = sub == n
                named = named + jnp.where(here & hit, 1.0, 0.0)
                gate = gate + jnp.where(here & hit, table[top + k : top + k + 1, :], 0.0)
        place = jnp.dot(named.astype(BF16), earlier, preferred_element_type=F32)
        for n in range(2):
            chosen = jnp.where(slots == place[n : n + 1, :], named[n : n + 1, :], 0.0)
            sel[at, n * capacity : (n + 1) * capacity] = chosen.astype(BF16)
            sel_back[2 * at + n] = chosen.T.astype(BF16)
        gate_cols[at] = gate.T

    def pick(at, block):
        return jnp.dot(sel[at], block, preferred_element_type=F32).astype(BF16)

    route(meta[...], 0)
    for c in range(parts):
        both = pick(0, normed_ref[:, cols_of(c)])
        rows_in[0, :, cols_of(c)] = both[:capacity]
        outbound[:, cols_of(c)] = both[capacity:]
    side_rows = send(outbound, rows_in.at[1], row_send, row_recv, {"ep": side})
    side_rows.start()

    def relay_of(slot, c):
        return send(
            relay_out.at[slot, :, cols_of(c)],
            rows_in.at[2 + slot, :, cols_of(c)],
            relay_send.at[slot],
            relay_recv.at[slot],
            {"ep": side},
        )

    def relay(slot, c):
        @pl.when(inner)
        def _():
            dense_of(slot, c).wait_recv()
            both = pick(1 + slot, dense_in[slot, :, cols_of(c)])
            relay_out[slot, :, cols_of(c)] = both[capacity:]
            relay_of(slot, c).start()
            rows_in[2 + slot, :, cols_of(c)] = both[:capacity]

    def forward(n):
        over_x(n).wait_recv()
        send(
            piece_of(n, 2, grp),
            piece_of(n, 2, grp),
            y_send.at[kind_of(n)],
            y_recv.at[n],
            {"grp": 1 - grp},
        ).start()
        cross_of(0, n).start()

    def cross_of(way, n):
        g = grp if way == 0 else 1 - grp
        landed = cross_wide.at[way, n % 2] if n < wide_cuts else cross_down.at[way, n - wide_cuts]
        return send(piece_of(n, 2, g), piece_of(n, 3, g), cross_send.at[way, kind_of(n)], landed, mate)

    def forward_again(n):
        arrived(piece_of(n, 2, 1 - grp), y_recv.at[n])
        cross_of(1, n).start()

    units = hid.shape[1] // 4

    def hidden(s, flat, rows):
        gate = jnp.dot(flat, g_all[s].reshape(deep, units), preferred_element_type=F32)
        up = jnp.dot(flat, u_all[s].reshape(deep, units), preferred_element_type=F32)
        hid[rows, s * units : (s + 1) * units] = (gate / (1.0 + jnp.exp(-gate)) * up).astype(BF16)

    early = 3 * capacity

    def hidden_early(s):
        hidden(s, rows_in[0:3].reshape(early, deep), slice(0, early))

    def hidden_late(s):
        hidden(s, rows_in[3], slice(early, early + capacity))

    relays = 2 * parts
    lag = 3
    when = {}
    for m in range(relays):
        when[2 * m + (2 if m < parts else 1)] = m

    for n in range(wide_cuts):
        if n in when:
            relay(when[n] // parts, when[n] % parts)
        forward(n)
        if n == 1:

            @pl.when(inner)
            def _():
                for slot in range(2):
                    arrived(meta_in.at[slot], meta_recv.at[slot])
                    route(meta_in[slot], 1 + slot)

        if n >= lag:
            forward_again(n - lag)

    pieces = (q_ref, k_ref, v_ref)
    dests = (
        far[1] * is_inner + side * (1 - is_inner),
        far[0] * is_inner + far[1] * (1 - is_inner),
        side * is_inner + far[0] * (1 - is_inner),
    )
    for r, dest in enumerate(dests):
        cols = pl.ds(pl.multiple_of(dest * width, width), width)
        for n in range(3):
            send(
                pieces[n].at[:, cols],
                qkv_all.at[me, n],
                pack_send,
                pack_recv.at[me],
                {"ep": dest},
            ).start()
        send(bias_ref, bias_all.at[me], bias_send.at[r], bias_recv.at[me], {"ep": dest}).start()

    side_rows.wait_recv()

    @pl.when(outside)
    def _():
        arrived(relay_out.at[0], relay_recv.at[0])

    hidden_early(0)
    forward_again(wide_cuts - 3)
    forward(wide_cuts)
    for copy in nears:
        copy.wait_recv()
    hidden_early(1)
    forward_again(wide_cuts - 2)
    forward(wide_cuts + 1)
    forward_again(wide_cuts - 1)
    hidden_early(2)
    forward(wide_cuts + 2)
    forward_again(wide_cuts)

    @pl.when(outside)
    def _():
        arrived(relay_out.at[1], relay_recv.at[1])

    for s in range(3):
        hidden_late(s)
    forward(wide_cuts + 3)
    forward_again(wide_cuts + 1)
    for n, r in enumerate((g_all, u_all)):
        arrived(r.at[3, grp], cross_wide.at[0, n])
        arrived(r.at[3, 1 - grp], cross_wide.at[1, n])
    hidden_early(3)
    hidden_late(3)

    def outer_of(c):
        cols = cols_of(c, fine)
        return send(
            outer_out.at[:, :, cols], outer_in.at[:, :, cols], outer_send, outer_recv.at[c], {"ep": side}
        )

    def final(c):
        cols = cols_of(c, fine)
        for way in range(2):
            cross_of(way, wide_cuts + c).wait_recv()
        down = jnp.concatenate(
            [d_all[s, :, :, cols].reshape(units, deep // fine) for s in range(4)], axis=0
        )
        whole = jnp.dot(hid[...], down, preferred_element_type=F32).astype(BF16)
        for slot in range(2):
            first = (2 + slot) * capacity
            outer_out[slot, :, cols] = whole[first : first + capacity]

        @pl.when(outside)
        def _():
            outer_of(c).start()

        back_out[:, cols] = whole[capacity : 2 * capacity]
        back_in[0, :, cols] = whole[:capacity]

    def home_of(slot, c):
        return send(
            dense_out.at[slot, :, cols_of(c, fine)],
            dense_back.at[:, cols_of(c, fine)],
            home_send.at[slot],
            home_recv.at[c],
            {"ep": far[slot]},
        )

    def weigh(at, near_rows, far_rows):
        gate = gate_cols[at]
        here = jnp.dot(sel_back[2 * at], near_rows, preferred_element_type=F32)
        there = jnp.dot(sel_back[2 * at + 1], far_rows, preferred_element_type=F32)
        return gate[:, 0:1] * here + gate[:, 1:2] * there

    def return_home(c):
        cols = cols_of(c, fine)

        @pl.when(inner)
        def _():
            outer_of(c).wait_recv()
            for slot in range(2):
                dense_out[slot, :, cols] = weigh(
                    1 + slot, outer_out[slot, :, cols], outer_in[slot, :, cols]
                ).astype(BF16)
                home_of(slot, c).start()

    block = (span, span)
    key_sub = lax.broadcasted_iota(jnp.int32, block, 0)
    key_lane = lax.broadcasted_iota(jnp.int32, block, 1)
    after = (key_sub > key_lane).astype(BF16)
    past = key_lane < key_sub

    def attend(i):
        result = []
        for h in range(heads):
            cols = slice(h * head, (h + 1) * head)
            query = qkv_all[i, 0][:, cols]
            for j in range(i, -1, -1):
                z = lax.dot_general(
                    query,
                    qkv_all[j, 1][:, cols],
                    (((1,), (1,)), ((), ())),
                    preferred_element_type=F32,
                )
                z = z * head ** (-0.5) + bias_rows[j, pl.ds(me * heads + h, 1), :]
                soft = jnp.log1p(jnp.exp(-jnp.abs(z)))
                rest = -(jnp.maximum(z, 0.0) + soft)
                stop = jnp.minimum(z, 0.0) - soft
                if j == i:
                    rest = jnp.where(past, rest, 0.0)
                hi = rest.astype(BF16)
                left = rest - hi.astype(F32)
                mid = left.astype(BF16)
                low = (left - mid.astype(F32)).astype(BF16)
                sums = jnp.dot(
                    jnp.concatenate([hi, mid, low], axis=0), after, preferred_element_type=F32
                )
                within = sums[:span] + sums[span : 2 * span] + sums[2 * span :]
                local = jnp.exp(stop + within)
                if j == i:
                    local = jnp.where(past, local, 0.0)
                part = jnp.dot(
                    local.astype(BF16), qkv_all[j, 2][:, cols], preferred_element_type=F32
                )
                total = part if j == i else total + jnp.exp(carry) * part
                if j > 0:
                    tally = jnp.sum(rest, axis=1, keepdims=True)
                    carry = tally if j == i else carry + tally
            result.append(total)
        got = jnp.concatenate(result, axis=1).astype(BF16)
        att_send[i] = got

        @pl.when(me == i)
        def _():
            att_all[i] = got

        @pl.when(me != i)
        def _():
            att_of(i, me).start()

    def att_of(i, j):
        return send(att_send.at[i], att_all.at[j], att_ssem.at[i], att_rsem.at[j], {"ep": i})

    final(0)
    forward(wide_cuts + 4)
    forward_again(wide_cuts + 2)
    final(1)
    forward(wide_cuts + 5)
    forward_again(wide_cuts + 3)
    final(2)
    forward(wide_cuts + 6)
    forward_again(wide_cuts + 4)
    final(3)
    for copy in mine:
        copy.wait()
    loads[8].wait()
    for r in range(1, ep):
        source = lax.rem(me + r, ep)
        arrived(qkv_all.at[source], pack_recv.at[source])
        arrived(bias_all.at[source], bias_recv.at[source])
    bias_rows[...] = bias_all[...].astype(F32)
    return_home(0)
    attend(3)
    forward(wide_cuts + 7)
    forward_again(wide_cuts + 5)
    final(4)
    return_home(1)
    attend(2)
    forward_again(wide_cuts + 6)
    final(5)
    return_home(2)
    attend(1)
    forward_again(wide_cuts + 7)
    final(6)
    return_home(3)
    attend(0)
    final(7)
    side_back = send(back_out, back_in.at[1], back_ssem, back_rsem, {"ep": side})
    side_back.start()
    for c in range(4, fine):
        return_home(c)
    for j in range(ep):

        @pl.when(me != j)
        def _():
            arrived(att_all.at[j], att_rsem.at[j])

    ow_copy.wait()
    attended = jnp.concatenate([att_all[j] for j in range(ep)], axis=1)
    term = jnp.dot(attended, ow[...], preferred_element_type=F32).astype(BF16)
    proj[...] = term.reshape(proj.shape)
    shares = [
        send(proj.at[mates[m]], proj_in.at[m], proj_ssem.at[m], proj_rsem.at[m], {"tp": mates[m]})
        for m in (2, 3, 1)
    ]
    for copy in shares:
        copy.start()
    whole = proj[tp].astype(F32)
    for copy in shares:
        copy.wait_recv()
    for m in (1, 2, 3):
        whole = whole + proj_in[m].astype(F32)
    loads[7].wait()
    scale = lax.rsqrt(jnp.mean(whole * whole, axis=-1, keepdims=True) + 1e-06)
    mixed_ref[...] = (whole * scale * mix_own[...]).astype(BF16)
    drained(normed_ref, dense_send)
    for n, r in enumerate((g_all, u_all, d_all)):
        drained(r.at[0, grp], x_send.at[n])
        drained(r.at[2, grp], y_send.at[n])
        drained(r.at[2, grp], cross_send.at[0, n])
        drained(r.at[2, 1 - grp], cross_send.at[1, n])
        nears[n].wait_send()
    drained(qkv_all.at[pl.ds(0, 3)], pack_send)
    for r in range(ep - 1):
        drained(bias_all.at[0], bias_send.at[r])
    side_rows.wait_send()
    drained(meta, meta_send)
    for i in range(ep):

        @pl.when(me != i)
        def _():
            drained(att_send.at[i], att_ssem.at[i])

    for copy in shares:
        copy.wait_send()
    side_back.wait_recv()
    for c in range(fine):
        cols = cols_of(c, fine)
        acc[:, cols] = weigh(0, back_in[0, :, cols], back_in[1, :, cols])
    side_back.wait_send()

    @pl.when(outside)
    def _():
        drained(outer_out, outer_send)

    for c in range(fine):
        cols = cols_of(c, fine)
        home_of(0, c).wait_recv()
        out_ref[:, cols] = (acc[:, cols] + dense_back[:, cols].astype(F32)).astype(BF16)

    @pl.when(inner)
    def _():
        for slot in range(2):
            drained(relay_out.at[slot], relay_send.at[slot])
            drained(dense_out.at[slot], home_send.at[slot])


def settle_kernel(mixed_ref, out_ref, mixed_to, out_to, sems):
    copies = [
        pltpu.make_async_copy(out_ref, out_to, sems.at[0]),
        pltpu.make_async_copy(mixed_ref, mixed_to, sems.at[1]),
    ]
    for copy in copies:
        copy.start()
    for copy in copies:
        copy.wait()


def fused_device(
    groups,
    ep,
    tp,
    queries,
    keys,
    values,
    stop_bias,
    out_weight,
    mix_gain,
    moe_input,
    ffn_gain,
    expert_ids,
    expert_scores,
    gate_weight,
    up_weight,
    down_weight,
):
    span, cols = queries.shape
    tokens, deep = moe_input.shape
    top = expert_ids.shape[1]
    capacity = 3 * tokens * top // (2 * ep)
    width = cols // ep
    heads = stop_bias.shape[1]
    units = gate_weight.shape[2]
    cuts = 8
    parts = 4
    fine = 8
    lines = 8
    gate = gate_weight.reshape(groups, cuts, deep // (groups * cuts), units)
    up = up_weight.reshape(gate.shape)
    down = down_weight.reshape(groups, units // groups, deep)
    chunks = 2 * cuts + fine
    vmem = pl.BlockSpec(memory_space=pltpu.VMEM)
    hbm = pl.BlockSpec(memory_space=pl.ANY)
    dma = pltpu.SemaphoreType.DMA
    results = pl.pallas_call(
        functools.partial(layer_kernel, ep, capacity, cols // heads),
        out_shape=(
            pltpu.VMEM((span // tp, deep), BF16),
            pltpu.VMEM((tokens, deep), BF16),
        ),
        in_specs=[hbm] * 13,
        out_specs=(vmem, vmem),
        scratch_shapes=[
            pltpu.VMEM((tokens, deep), BF16),
            pltpu.VMEM((1, deep), F32),
            pltpu.VMEM((1, deep), F32),
            pltpu.VMEM((top, tokens), jnp.int32),
            pltpu.VMEM((top, tokens), F32),
            pltpu.VMEM((ep, 3, span, width), BF16),
            pltpu.VMEM((ep, heads, span), BF16),
            pltpu.VMEM((ep, heads, span), F32),
            pltpu.VMEM((ep, span, width), BF16),
            pltpu.VMEM((ep, span, width), BF16),
            pltpu.VMEM((tp, span // tp, deep), BF16),
            pltpu.VMEM((tp, span // tp, deep), BF16),
            pltpu.VMEM(out_weight.shape, BF16),
            pltpu.VMEM((lines, tokens), F32),
            pltpu.VMEM((2, lines, tokens), F32),
            pltpu.VMEM((tokens, deep), BF16),
            pltpu.VMEM((2, tokens, deep), BF16),
            pltpu.VMEM((3, 2 * capacity, tokens), BF16),
            pltpu.VMEM((6, tokens, capacity), BF16),
            pltpu.VMEM((3, tokens, tokens), F32),
            pltpu.VMEM((capacity, deep), BF16),
            pltpu.VMEM((2, capacity, deep), BF16),
            pltpu.VMEM((ep, capacity, deep), BF16),
            pltpu.VMEM((ep * capacity, tp * units), BF16),
            pltpu.VMEM((tokens, deep), F32),
            pltpu.VMEM((capacity, deep), BF16),
            pltpu.VMEM((2, capacity, deep), BF16),
            pltpu.VMEM((2, capacity, deep), BF16),
            pltpu.VMEM((2, capacity, deep), BF16),
            pltpu.VMEM((2, tokens, deep), BF16),
            pltpu.VMEM((tokens, deep), BF16),
            pltpu.VMEM((4,) + gate.shape, BF16),
            pltpu.VMEM((4,) + up.shape, BF16),
            pltpu.VMEM((4,) + down.shape, BF16),
            dma((9,)),
            dma((3,)),
            dma(()),
            dma(()),
            dma((ep,)),
            dma((ep,)),
            dma((ep,)),
            dma(()),
            dma(()),
            dma(()),
            dma((2,)),
            dma(()),
            dma((2, parts)),
            dma((2,)),
            dma((2,)),
            dma((ep,)),
            dma((ep,)),
            dma(()),
            dma(()),
            dma(()),
            dma((fine,)),
            dma((2,)),
            dma((fine,)),
            dma((tp,)),
            dma((tp,)),
            dma((3,)),
            dma((3,)),
            dma((3,)),
            dma((chunks,)),
            dma((3,)),
            dma((chunks,)),
            dma((2, 3)),
            dma((2, 2)),
            dma((2, fine)),
        ],
        compiler_params=pltpu.CompilerParams(
            collective_id=0, has_side_effects=True, vmem_limit_bytes=60 * 2**20
        ),
    )(
        queries,
        keys,
        values,
        stop_bias.T,
        out_weight,
        mix_gain.reshape(1, deep),
        moe_input,
        ffn_gain.reshape(1, deep),
        expert_ids.T,
        expert_scores.T,
        gate,
        up,
        down,
    )
    results = [pltpu.with_memory_space_constraint(r, pltpu.VMEM) for r in results]
    return pl.pallas_call(
        settle_kernel,
        out_shape=tuple(jax.ShapeDtypeStruct(r.shape, r.dtype) for r in results),
        in_specs=[vmem] * 2,
        out_specs=(hbm, hbm),
        scratch_shapes=[dma((2,))],
    )(*results)


def pick_plan(groups, ep, tp, *args):
    heads = args[3].shape[1]
    width = args[0].shape[1] // ep
    if groups == 2 and tp == 4 and ep == 4 and heads % ep == 0 and width % 128 == 0:
        return fused_device(groups, ep, tp, *args)
    return per_device(*args)


def solution(mesh):
    return jax.shard_map(
        functools.partial(pick_plan, mesh.shape["grp"], mesh.shape["ep"], mesh.shape["tp"]),
        mesh=mesh,
        in_specs=(
            P(("grp", "ep"), "tp"),
            P(("grp", "ep"), "tp"),
            P(("grp", "ep"), "tp"),
            P(("grp", "ep"), "tp"),
            P("tp", None),
            P(),
            P(("grp", "ep", "tp"), None),
            P(),
            P(("grp", "ep", "tp"), None),
            P(("grp", "ep", "tp"), None),
            P("ep", None, "tp"),
            P("ep", None, "tp"),
            P("ep", "tp", None),
        ),
        out_specs=(P(("grp", "ep", "tp"), None), P(("grp", "ep", "tp"), None)),
        check_vma=False,
    )
```

```python
import functools

import jax
import jax.numpy as jnp
from jax import lax
from jax.experimental import pallas as pl
from jax.experimental.pallas import tpu as pltpu
from jax.sharding import PartitionSpec as P

MESH = pl.DeviceIdType.MESH
F32 = jnp.float32
BF16 = jnp.bfloat16


def norm_rows(values, gain):
    values = values.astype(jnp.float32)
    scale = lax.rsqrt(jnp.mean(values * values, axis=-1, keepdims=True) + 1e-06)
    return values * scale * gain


def break_terms(query_heads, query_place, key_block, bias_block, first):
    span = key_block.shape[0]
    heads = query_heads.shape[1]
    key_heads = key_block.reshape(span, heads, -1)
    scores = jnp.einsum("qhd,khd->hqk", query_heads, key_heads, preferred_element_type=jnp.float32)
    scores = scores * query_heads.shape[2] ** (-0.5) + bias_block.astype(jnp.float32).T[:, None, :]
    key_place = first + jnp.arange(span)
    past = (key_place[None, :] < query_place[:, None])[None]
    rest = jnp.where(past, jax.nn.log_sigmoid(-scores), 0.0)
    later = lax.cumsum(rest, axis=2, reverse=True)
    return (scores, past, rest, later)


def block_part(scores, past, rest, later, value_block, heads):
    within = later - rest
    local = jnp.where(past, jnp.exp(jax.nn.log_sigmoid(scores) + within), 0.0).astype(jnp.bfloat16)
    span = value_block.shape[0]
    value_heads = value_block.reshape(span, heads, -1)
    part = jnp.einsum("hqk,khd->qhd", local, value_heads, preferred_element_type=jnp.float32)
    return part.reshape(part.shape[0], -1)


def keep(state):
    return state


def dispatch_plan(normed, expert_ids, experts, capacity):
    rows, top = expert_ids.shape
    flat_ids = expert_ids.reshape(rows * top)
    onehot = (flat_ids[:, None] == jnp.arange(experts)[None, :]).astype(jnp.int32)
    earlier = jnp.cumsum(onehot, axis=0) - onehot
    place = jnp.sum(earlier * onehot, axis=1)
    target = flat_ids * capacity + place
    source = (
        jnp.zeros((experts * capacity,), jnp.int32)
        .at[target]
        .set(jnp.arange(rows * top, dtype=jnp.int32) // top + 1)
    )
    padded = jnp.concatenate([jnp.zeros((1, normed.shape[1]), normed.dtype), normed], axis=0)
    return (padded[source].reshape(experts, capacity, normed.shape[1]), target)


def expert_hidden(piece, gate_weight, up_weight):
    flat = piece.reshape(-1, piece.shape[-1])
    gate = jnp.dot(flat, gate_weight[0], preferred_element_type=jnp.float32)
    upward = jnp.dot(flat, up_weight[0], preferred_element_type=jnp.float32)
    hidden = (jax.nn.silu(gate) * upward).astype(jnp.bfloat16)
    return hidden.reshape(piece.shape[0], piece.shape[1], -1)


def send_back(summed):
    return lax.all_to_all(
        summed.astype(jnp.bfloat16), "ep", split_axis=0, concat_axis=0, tiled=True
    )


def return_rows(hidden_all, down_weight, sources):
    flat = hidden_all.reshape(-1, hidden_all.shape[2])
    product = jnp.dot(flat, down_weight[0], preferred_element_type=jnp.float32)
    return send_back(
        lax.psum_scatter(
            product.reshape(sources * lax.axis_size("tp"), hidden_all.shape[1], -1).astype(
                jnp.bfloat16
            ),
            "tp",
            scatter_dimension=0,
            tiled=True,
        ).astype(jnp.float32)
    )


def per_device(
    queries,
    keys,
    values,
    stop_bias,
    out_weight,
    mix_gain,
    moe_input,
    ffn_gain,
    expert_ids,
    expert_scores,
    gate_weight,
    up_weight,
    down_weight,
):
    span = queries.shape[0]
    heads = stop_bias.shape[1]
    width_heads = queries.shape[1]
    blocks = lax.axis_size("ep")
    own_first = lax.axis_index("ep") * span
    query_heads = queries.reshape(span, heads, -1)
    query_place = own_first + jnp.arange(span)

    def piece_rows(piece, index):
        return tuple((lax.dynamic_slice_in_dim(member, index * span, span, 0) for member in piece))

    start_state = (
        jnp.zeros((blocks, heads, span), jnp.float32),
        jnp.zeros((blocks, span, width_heads), jnp.float32),
    )
    piece = (
        lax.all_gather(keys, "ep", axis=0, tiled=True),
        lax.all_gather(values, "ep", axis=0, tiled=True),
        lax.all_gather(stop_bias, "ep", axis=0, tiled=True),
    )

    def one_block(index, state):
        key_block, value_block, bias_block = piece_rows(piece, index)
        first = index * span

        def compute(inner_state):
            totals, parts = inner_state
            scores, past, rest, later = break_terms(
                query_heads, query_place, key_block, bias_block, first
            )
            part = block_part(scores, past, rest, later, value_block, heads)
            number = first // span
            totals = lax.dynamic_update_index_in_dim(totals, later[:, :, 0], number, 0)
            parts = lax.dynamic_update_index_in_dim(parts, part, number, 0)
            return (totals, parts)

        return lax.cond(first <= own_first, compute, keep, state)

    totals, parts = lax.fori_loop(0, piece[0].shape[0] // span, one_block, start_state)
    carried = lax.cumsum(totals, axis=0, reverse=True) - totals
    factor = jnp.exp(carried).transpose(0, 2, 1)[:, :, :, None]
    attended = jnp.sum(factor * parts.reshape(blocks, span, heads, -1), axis=0).reshape(
        span, width_heads
    )
    attended = attended.astype(jnp.bfloat16)
    projected = lax.psum_scatter(
        jnp.dot(attended, out_weight, preferred_element_type=jnp.float32).astype(jnp.bfloat16),
        "tp",
        scatter_dimension=0,
        tiled=True,
    ).astype(jnp.float32)
    mixed = norm_rows(projected, mix_gain).astype(jnp.bfloat16)
    normed = norm_rows(moe_input, ffn_gain).astype(jnp.bfloat16)
    rows, top = expert_ids.shape
    experts = lax.axis_size("ep")
    capacity = 3 * rows * top // (2 * experts)
    weights = expert_scores / jnp.sum(expert_scores, axis=1, keepdims=True)
    outbound, target = dispatch_plan(normed, expert_ids, experts, capacity)
    arrived = lax.all_to_all(outbound, "ep", split_axis=0, concat_axis=0, tiled=True)
    hidden_all = expert_hidden(
        lax.all_gather(arrived, "tp", axis=0, tiled=True), gate_weight, up_weight
    )
    returned = return_rows(hidden_all, down_weight, arrived.shape[0])
    picked = returned.reshape(experts * capacity, -1)[target].reshape(rows, top, -1)
    experts_mixed = jnp.sum(picked.astype(jnp.float32) * weights[:, :, None], axis=1).astype(
        jnp.bfloat16
    )
    return (mixed, experts_mixed)


def layer_kernel(
    ep,
    capacity,
    head,
    q_ref,
    k_ref,
    v_ref,
    bias_ref,
    ow_ref,
    mix_gain_ref,
    x_ref,
    ffn_gain_ref,
    ids_ref,
    scores_ref,
    g_ref,
    u_ref,
    d_ref,
    mixed_ref,
    out_ref,
    x_own,
    gain_own,
    mix_own,
    ids_own,
    scores_own,
    qkv_all,
    bias_all,
    bias_rows,
    att_send,
    att_all,
    proj,
    proj_in,
    ow,
    meta,
    meta_in,
    normed_ref,
    dense_in,
    sel,
    sel_back,
    gate_cols,
    outbound,
    relay_out,
    rows_in,
    hid,
    sofar,
    acc,
    back_out,
    back_in,
    outer_out,
    outer_in,
    dense_out,
    dense_back,
    g_all,
    u_all,
    d_all,
    load_sem,
    own_sem,
    ow_sem,
    pack_send,
    pack_recv,
    bias_send,
    bias_recv,
    row_send,
    row_recv,
    meta_send,
    meta_recv,
    dense_send,
    dense_recv,
    relay_send,
    relay_recv,
    att_ssem,
    att_rsem,
    back_ssem,
    back_rsem,
    outer_send,
    outer_recv,
    home_send,
    home_recv,
    proj_ssem,
    proj_rsem,
    near_send,
    near_recv,
    x_send,
    x_recv,
    y_send,
    y_recv,
    cross_send,
    cross_wide,
    cross_down,
):
    me = lax.axis_index("ep")
    tp = lax.axis_index("tp")
    grp = lax.axis_index("grp")
    chip, core = tp // 2, tp % 2
    mates = [None, chip * 2 + (1 - core), (1 - chip) * 2 + core, (1 - chip) * 2 + (1 - core)]
    span = q_ref.shape[0]
    width = qkv_all.shape[3]
    heads = width // head
    tokens, deep = x_ref.shape
    top = ids_ref.shape[0]
    parts = dense_recv.shape[1]
    fine = home_recv.shape[0]
    wide_cuts = 2 * g_ref.shape[1]

    half = me // 2
    is_inner = lax.rem(me + 1, ep) // 2
    inner = is_inner == 1
    outside = is_inner == 0
    side = me + 1 - 2 * (me % 2)
    far = (3 * (1 - half), 2 - half)

    loads = [
        pltpu.make_async_copy(s, t, load_sem.at[n])
        for n, (s, t) in enumerate(
            (
                (x_ref, x_own),
                (ids_ref, ids_own),
                (scores_ref, scores_own),
                (ffn_gain_ref, gain_own),
                (g_ref, g_all.at[0]),
                (u_ref, u_all.at[0]),
                (d_ref, d_all.at[0]),
                (mix_gain_ref, mix_own),
                (bias_ref, bias_all.at[me]),
            )
        )
    ]
    own = pl.ds(pl.multiple_of(me * width, width), width)
    mine = [
        pltpu.make_async_copy(r.at[:, own], qkv_all.at[me, n], own_sem.at[n])
        for n, r in enumerate((q_ref, k_ref, v_ref))
    ]
    ow_copy = pltpu.make_async_copy(ow_ref, ow, ow_sem)
    for copy in loads:
        copy.start()

    barrier = pltpu.get_barrier_semaphore()
    peers = [{"ep": lax.rem(me + r, ep)} for r in range(1, ep)]
    peers += [{"tp": mates[m]} for m in (1, 2, 3)] + [{"grp": 1 - grp}]
    for peer in peers:
        pl.semaphore_signal(barrier, inc=1, device_id=peer, device_id_type=MESH)
    for copy in mine:
        copy.start()
    ow_copy.start()

    def send(src, dst, ssem, rsem, peer):
        return pltpu.make_async_remote_copy(
            src_ref=src,
            dst_ref=dst,
            send_sem=ssem,
            recv_sem=rsem,
            device_id=peer,
            device_id_type=MESH,
        )

    mate = {"tp": mates[1]}

    def arrived(ref, sem):
        send(ref, ref, sem, sem, mate).wait_recv()

    def drained(ref, sem):
        send(ref, ref, sem, sem, mate).wait_send()

    def cols_of(c):
        return slice(c * (deep // parts), (c + 1) * (deep // parts))

    def strip(c):
        unit = deep // (2 * (fine - 1))
        edges = [0, 1] + [2 * n for n in range(1, fine)]
        return slice(edges[c] * unit, edges[c + 1] * unit)

    def piece_of(n, s, g):
        if n < wide_cuts:
            return (g_all, u_all)[n % 2].at[s, g, n // 2]
        return d_all.at[s, g, :, strip(n - wide_cuts)]

    def kind_of(n):
        return n % 2 if n < wide_cuts else 2

    chunks = wide_cuts + fine

    for n in range(4):
        loads[n].wait()
    gates = scores_own[...]
    gates = gates / jnp.sum(gates, axis=0, keepdims=True)
    meta[...] = jnp.zeros_like(meta)
    meta[0:top] = ids_own[...].astype(F32)
    meta[top : 2 * top] = gates
    values = x_own[...].astype(F32)
    scale = lax.rsqrt(jnp.mean(values * values, axis=-1, keepdims=True) + 1e-06)
    normed_ref[...] = (values * scale * gain_own[...]).astype(BF16)

    pl.semaphore_wait(barrier, len(peers))

    def over_x(n):
        return send(
            piece_of(n, 0, grp),
            piece_of(n, 2, grp),
            x_send.at[kind_of(n)],
            x_recv.at[n],
            {"tp": mates[2]},
        )

    loads[4].wait()
    over_x(0).start()
    send(meta, meta_in.at[is_inner], meta_send, meta_recv.at[is_inner], {"ep": far[1]}).start()

    def dense_of(slot, c):
        return send(
            normed_ref.at[:, cols_of(c)],
            dense_in.at[slot, :, cols_of(c)],
            dense_send,
            dense_recv.at[slot, c],
            {"ep": far[1]},
        )

    pieces = (q_ref, k_ref, v_ref)

    def pack(r, dest):
        cols = pl.ds(pl.multiple_of(dest * width, width), width)
        for n in range(3):
            send(
                pieces[n].at[:, cols],
                qkv_all.at[me, n],
                pack_send,
                pack_recv.at[me],
                {"ep": dest},
            ).start()
        send(bias_ref, bias_all.at[me], bias_send.at[r], bias_recv.at[me], {"ep": dest}).start()

    @pl.when(inner)
    def _():
        pack(0, far[1])
        pack(1, far[0])

    for c in range(parts):
        dense_of(is_inner, c).start()

    @pl.when(outside)
    def _():
        pack(0, far[1])
        pack(1, far[0])
        pack(2, side)

    loads[5].wait()
    for n in range(1, wide_cuts):
        over_x(n).start()
    loads[6].wait()
    for n in range(wide_cuts, chunks):
        over_x(n).start()
    nears = [
        send(r.at[0], r.at[1], near_send.at[n], near_recv.at[n], mate)
        for n, r in enumerate((g_all, u_all, d_all))
    ]
    square = (tokens, tokens)
    lane = lax.broadcasted_iota(jnp.int32, square, 1)
    sub = lax.broadcasted_iota(jnp.int32, square, 0)
    earlier = (sub < lane).astype(BF16)
    slots = lax.broadcasted_iota(jnp.int32, (capacity, tokens), 0).astype(F32)

    def route(table, at):
        named = jnp.zeros(square, F32)
        gate = jnp.zeros(square, F32)
        for n, e in enumerate((me, side)):
            place_of = e.astype(F32)
            for k in range(top):
                hit = table[k : k + 1, :] == place_of
                here = sub == n
                named = named + jnp.where(here & hit, 1.0, 0.0)
                gate = gate + jnp.where(here & hit, table[top + k : top + k + 1, :], 0.0)
        place = jnp.dot(named.astype(BF16), earlier, preferred_element_type=F32)
        for n in range(2):
            chosen = jnp.where(slots == place[n : n + 1, :], named[n : n + 1, :], 0.0)
            sel[at, n * capacity : (n + 1) * capacity] = chosen.astype(BF16)
            sel_back[2 * at + n] = chosen.T.astype(BF16)
        gate_cols[at] = gate.T

    def pick(at, block):
        return jnp.dot(sel[at], block, preferred_element_type=F32).astype(BF16)

    route(meta[...], 0)
    for c in range(parts):
        both = pick(0, normed_ref[:, cols_of(c)])
        rows_in[0, :, cols_of(c)] = both[:capacity]
        outbound[:, cols_of(c)] = both[capacity:]
    side_rows = send(outbound, rows_in.at[1], row_send, row_recv, {"ep": side})
    side_rows.start()

    def relay_of(slot, c):
        return send(
            relay_out.at[slot, :, cols_of(c)],
            rows_in.at[2 + slot, :, cols_of(c)],
            relay_send.at[slot],
            relay_recv.at[slot],
            {"ep": side},
        )

    def relay(slot, c):
        @pl.when(inner)
        def _():
            if c == 0:
                arrived(meta_in.at[slot], meta_recv.at[slot])
                route(meta_in[slot], 1 + slot)
            dense_of(slot, c).wait_recv()
            both = pick(1 + slot, dense_in[slot, :, cols_of(c)])
            relay_out[slot, :, cols_of(c)] = both[capacity:]
            relay_of(slot, c).start()
            rows_in[2 + slot, :, cols_of(c)] = both[:capacity]

    def forward(n):
        over_x(n).wait_recv()
        send(
            piece_of(n, 2, grp),
            piece_of(n, 2, grp),
            y_send.at[kind_of(n)],
            y_recv.at[n],
            {"grp": 1 - grp},
        ).start()
        cross_of(0, n).start()

    def cross_of(way, n):
        g = grp if way == 0 else 1 - grp
        landed = cross_wide.at[way, n % 2] if n < wide_cuts else cross_down.at[n - wide_cuts]
        return send(piece_of(n, 2, g), piece_of(n, 3, g), cross_send.at[way, kind_of(n)], landed, mate)

    def forward_again(n):
        arrived(piece_of(n, 2, 1 - grp), y_recv.at[n])
        cross_of(1, n).start()

    units = hid.shape[1] // 4

    depth = deep // 2

    def rows_of(a, b):
        return slice(a * capacity, b * capacity)

    def activate(gate, up, s, rows):
        hid[rows, s * units : (s + 1) * units] = (gate / (1.0 + jnp.exp(-gate)) * up).astype(BF16)

    def hidden(s, a, b):
        flat = rows_in[a:b].reshape((b - a) * capacity, deep)
        gate = jnp.dot(flat, g_all[s].reshape(deep, units), preferred_element_type=F32)
        up = jnp.dot(flat, u_all[s].reshape(deep, units), preferred_element_type=F32)
        activate(gate, up, s, rows_of(a, b))

    def hidden_early(s):
        hidden(s, 0, 3)

    def hidden_late(s):
        hidden(s, 3, 4)

    def half_of(s, g):
        cols = pl.ds(pl.multiple_of(g * depth, depth), depth)
        flat = rows_in[0:3, :, cols].reshape(3 * capacity, depth)
        gate = jnp.dot(flat, g_all[s, g].reshape(depth, units), preferred_element_type=F32)
        up = jnp.dot(flat, u_all[s, g].reshape(depth, units), preferred_element_type=F32)
        return gate, up

    def hidden_first(s):
        gate, up = half_of(s, grp)
        sofar[s - 2, 0] = gate
        sofar[s - 2, 1] = up

    def hidden_second(s):
        gate, up = half_of(s, 1 - grp)
        activate(sofar[s - 2, 0] + gate, sofar[s - 2, 1] + up, s, rows_of(0, 3))

    block = (span, span)
    key_sub = lax.broadcasted_iota(jnp.int32, block, 0)
    key_lane = lax.broadcasted_iota(jnp.int32, block, 1)
    after = (key_sub > key_lane).astype(BF16)
    past = key_lane < key_sub

    def attend(i, heads_now):
        for h in heads_now:
            cols = slice(h * head, (h + 1) * head)
            query = qkv_all[i, 0][:, cols] * BF16(head**-0.5)
            for j in range(i, -1, -1):
                z = lax.dot_general(
                    query,
                    qkv_all[j, 1][:, cols],
                    (((1,), (1,)), ((), ())),
                    preferred_element_type=F32,
                )
                z = z + bias_rows[j, pl.ds(me * heads + h, 1), :]
                stop = jnp.minimum(z, 0.0) - jnp.log(1.0 + jnp.exp(jnp.minimum(z, -z)))
                rest = stop - z
                if j == i:
                    rest = jnp.where(past, rest, 0.0)
                hi = rest.astype(BF16)
                left = rest - hi.astype(F32)
                mid = left.astype(BF16)
                low = (left - mid.astype(F32)).astype(BF16)
                sums = jnp.dot(
                    jnp.concatenate([hi, mid, low], axis=0), after, preferred_element_type=F32
                )
                within = sums[:span] + sums[span : 2 * span] + sums[2 * span :]
                local = jnp.exp(stop + within)
                if j == i:
                    local = jnp.where(past, local, 0.0)
                part = jnp.dot(
                    local.astype(BF16), qkv_all[j, 2][:, cols], preferred_element_type=F32
                )
                total = part if j == i else total + jnp.exp(carry) * part
                if j > 0:
                    tally = jnp.sum(rest, axis=1, keepdims=True)
                    carry = tally if j == i else carry + tally
            att_send[i, :, cols] = total.astype(BF16)
        if heads_now[-1] != heads - 1:
            return

        @pl.when(me == i)
        def _():
            att_all[i] = att_send[i]

        @pl.when(me != i)
        def _():
            att_of(i, me).start()

    def att_of(i, j):
        return send(att_send.at[i], att_all.at[j], att_ssem.at[i], att_rsem.at[j], {"ep": i})

    def packs_here():
        for copy in mine:
            copy.wait()
        loads[8].wait()
        for r in range(1, ep):
            source = lax.rem(me + r, ep)
            arrived(qkv_all.at[source], pack_recv.at[source])
            arrived(bias_all.at[source], bias_recv.at[source])
        bias_rows[...] = bias_all[...].astype(F32)

    firsts, lasts = tuple(range(heads // 2)), tuple(range(heads // 2, heads))
    everyone = firsts + lasts
    W = wide_cuts
    lag = 3
    near_at = (4, 7, 10)
    for n in range(W):
        if n % 2 == 0 and 2 <= n < 2 + 2 * parts:
            relay(0, n // 2 - 1)
        forward(n)
        if n >= lag:
            forward_again(n - lag)
        if n in near_at:
            nears[near_at.index(n)].start()
        if n == 9:

            @pl.when(inner)
            def _():
                pack(2, side)

        if n == 13:
            packs_here()
            attend(3, firsts)
        if n == 14:
            attend(3, lasts)
        if n == 15:
            relay(1, 0)
            attend(0, everyone)

    forward_again(W - 3)
    forward(W)
    attend(2, everyone)
    relay(1, 1)
    forward(W + 1)
    forward_again(W - 2)
    side_rows.wait_recv()

    @pl.when(outside)
    def _():
        arrived(relay_out.at[0], relay_recv.at[0])

    hidden_early(0)
    forward(W + 2)
    for copy in nears:
        copy.wait_recv()
    hidden_early(1)
    forward_again(W - 1)
    for n, r in enumerate((g_all, u_all)):
        arrived(r.at[3, grp], cross_wide.at[0, n])
    hidden_first(2)
    hidden_first(3)
    forward(W + 3)
    hidden_second(2)
    forward_again(W)
    relay(1, 2)
    forward(W + 4)
    for n, r in enumerate((g_all, u_all)):
        arrived(r.at[3, 1 - grp], cross_wide.at[1, n])
    hidden_second(3)
    forward_again(W + 1)

    def outer_of(slot, c):
        cols = strip(c)
        return send(
            outer_out.at[slot, :, cols],
            outer_in.at[slot, :, cols],
            outer_send.at[slot],
            outer_recv.at[slot, c],
            {"ep": side},
        )

    def back_of(cols):
        return send(
            back_out.at[:, cols], back_in.at[1, :, cols], back_ssem, back_rsem, {"ep": side}
        )

    def lower(cols, a, b):
        down = jnp.concatenate(
            [d_all[s, :, :, cols].reshape(units, -1) for s in range(4)], axis=0
        )
        return jnp.dot(hid[rows_of(a, b)], down, preferred_element_type=F32).astype(BF16)

    def put_far(slot, c, rows):
        outer_out[slot, :, strip(c)] = rows

        @pl.when(outside)
        def _():
            outer_of(slot, c).start()

    def final(c):
        cols = strip(c)
        arrived(d_all.at[3, :, :, cols], cross_down.at[c])
        rows = lower(cols, 0, 3)
        put_far(0, c, rows[rows_of(2, 3)])
        back_in[0, :, cols] = rows[rows_of(0, 1)]
        back_out[:, cols] = rows[rows_of(1, 2)]

        @pl.when(inner)
        def _():
            back_of(cols).start()

    def final_late(c):
        put_far(1, c, lower(strip(c), 3, 4))

    def back_strips(first, last):
        @pl.when(outside)
        def _():
            back_of(slice(strip(first).start, strip(last).stop)).start()

    def home_of(slot, c):
        return send(
            dense_out.at[slot, :, strip(c)],
            dense_back.at[:, strip(c)],
            home_send.at[slot],
            home_recv.at[c],
            {"ep": far[slot]},
        )

    def weigh(at, near_rows, far_rows):
        gate = gate_cols[at]
        here = jnp.dot(sel_back[2 * at], near_rows, preferred_element_type=F32)
        there = jnp.dot(sel_back[2 * at + 1], far_rows, preferred_element_type=F32)
        return gate[:, 0:1] * here + gate[:, 1:2] * there

    def return_home(slot, c):
        cols = strip(c)

        @pl.when(inner)
        def _():
            outer_of(slot, c).wait_recv()
            dense_out[slot, :, cols] = weigh(
                1 + slot, outer_out[slot, :, cols], outer_in[slot, :, cols]
            ).astype(BF16)
            home_of(slot, c).start()

    final(0)
    forward(W + 5)
    forward_again(W + 2)
    final(1)
    relay(1, 3)
    attend(1, everyone)
    forward(W + 6)
    forward_again(W + 3)
    final(2)
    return_home(0, 0)
    return_home(0, 1)
    forward(W + 7)
    forward_again(W + 4)
    final(3)
    return_home(0, 2)
    forward(W + 8)
    forward_again(W + 5)
    final(4)
    back_strips(0, 1)
    return_home(0, 3)
    forward_again(W + 6)
    final(5)
    return_home(0, 4)
    forward_again(W + 7)
    final(6)
    back_strips(2, 2)

    @pl.when(outside)
    def _():
        arrived(relay_out.at[1], relay_recv.at[1])

    hidden_late(0)
    return_home(0, 5)
    hidden_late(1)
    forward_again(W + 8)
    final(7)
    hidden_late(2)
    return_home(0, 6)
    hidden_late(3)
    final(8)
    back_strips(3, 3)
    final_late(0)
    final_late(1)
    return_home(0, 7)
    final_late(2)
    final_late(3)
    return_home(0, 8)
    final_late(4)
    return_home(1, 0)
    final_late(5)
    return_home(1, 1)
    for c in range(6, fine):
        final_late(c)
    back_strips(4, fine - 1)
    return_home(1, 2)
    for j in range(ep):

        @pl.when(me != j)
        def _():
            arrived(att_all.at[j], att_rsem.at[j])

    ow_copy.wait()
    attended = jnp.concatenate([att_all[j] for j in range(ep)], axis=1)
    term = jnp.dot(attended, ow[...], preferred_element_type=F32).astype(BF16)
    proj[...] = term.reshape(proj.shape)
    shares = [
        send(proj.at[mates[m]], proj_in.at[m], proj_ssem.at[m], proj_rsem.at[m], {"tp": mates[m]})
        for m in (2, 3, 1)
    ]
    for copy in shares:
        copy.start()
    for c in range(3, fine):
        return_home(1, c)
    whole = proj[tp].astype(F32)
    for copy in shares:
        copy.wait_recv()
    for m in (1, 2, 3):
        whole = whole + proj_in[m].astype(F32)
    loads[7].wait()
    scale = lax.rsqrt(jnp.mean(whole * whole, axis=-1, keepdims=True) + 1e-06)
    mixed_ref[...] = (whole * scale * mix_own[...]).astype(BF16)
    drained(normed_ref, dense_send)
    for n, r in enumerate((g_all, u_all, d_all)):
        drained(r.at[0, grp], x_send.at[n])
        drained(r.at[2, grp], y_send.at[n])
        drained(r.at[2, grp], cross_send.at[0, n])
        drained(r.at[2, 1 - grp], cross_send.at[1, n])
        nears[n].wait_send()
    drained(qkv_all.at[pl.ds(0, 3)], pack_send)
    for r in range(ep - 1):
        drained(bias_all.at[0], bias_send.at[r])
    side_rows.wait_send()
    drained(meta, meta_send)
    for i in range(ep):

        @pl.when(me != i)
        def _():
            drained(att_send.at[i], att_ssem.at[i])

    for copy in shares:
        copy.wait_send()
    arrived(back_out, back_rsem)
    for c in range(fine):
        cols = strip(c)
        acc[:, cols] = weigh(0, back_in[0, :, cols], back_in[1, :, cols])
    drained(back_out, back_ssem)

    @pl.when(outside)
    def _():
        for slot in range(2):
            drained(outer_out.at[slot], outer_send.at[slot])

    for c in range(fine):
        cols = strip(c)
        home_of(0, c).wait_recv()
        out_ref[:, cols] = (acc[:, cols] + dense_back[:, cols].astype(F32)).astype(BF16)

    @pl.when(inner)
    def _():
        for slot in range(2):
            drained(relay_out.at[slot], relay_send.at[slot])
            drained(dense_out.at[slot], home_send.at[slot])


def settle_kernel(mixed_ref, out_ref, mixed_to, out_to, sems):
    copies = [
        pltpu.make_async_copy(out_ref, out_to, sems.at[0]),
        pltpu.make_async_copy(mixed_ref, mixed_to, sems.at[1]),
    ]
    for copy in copies:
        copy.start()
    for copy in copies:
        copy.wait()


def fused_device(
    groups,
    ep,
    tp,
    queries,
    keys,
    values,
    stop_bias,
    out_weight,
    mix_gain,
    moe_input,
    ffn_gain,
    expert_ids,
    expert_scores,
    gate_weight,
    up_weight,
    down_weight,
):
    span, cols = queries.shape
    tokens, deep = moe_input.shape
    top = expert_ids.shape[1]
    capacity = 3 * tokens * top // (2 * ep)
    width = cols // ep
    heads = stop_bias.shape[1]
    units = gate_weight.shape[2]
    cuts = 8
    parts = 4
    fine = 9
    lines = 8
    gate = gate_weight.reshape(groups, cuts, deep // (groups * cuts), units)
    up = up_weight.reshape(gate.shape)
    down = down_weight.reshape(groups, units // groups, deep)
    chunks = 2 * cuts + fine
    vmem = pl.BlockSpec(memory_space=pltpu.VMEM)
    hbm = pl.BlockSpec(memory_space=pl.ANY)
    dma = pltpu.SemaphoreType.DMA
    results = pl.pallas_call(
        functools.partial(layer_kernel, ep, capacity, cols // heads),
        out_shape=(
            pltpu.VMEM((span // tp, deep), BF16),
            pltpu.VMEM((tokens, deep), BF16),
        ),
        in_specs=[hbm] * 13,
        out_specs=(vmem, vmem),
        scratch_shapes=[
            pltpu.VMEM((tokens, deep), BF16),
            pltpu.VMEM((1, deep), F32),
            pltpu.VMEM((1, deep), F32),
            pltpu.VMEM((top, tokens), jnp.int32),
            pltpu.VMEM((top, tokens), F32),
            pltpu.VMEM((ep, 3, span, width), BF16),
            pltpu.VMEM((ep, heads, span), BF16),
            pltpu.VMEM((ep, heads, span), F32),
            pltpu.VMEM((ep, span, width), BF16),
            pltpu.VMEM((ep, span, width), BF16),
            pltpu.VMEM((tp, span // tp, deep), BF16),
            pltpu.VMEM((tp, span // tp, deep), BF16),
            pltpu.VMEM(out_weight.shape, BF16),
            pltpu.VMEM((lines, tokens), F32),
            pltpu.VMEM((2, lines, tokens), F32),
            pltpu.VMEM((tokens, deep), BF16),
            pltpu.VMEM((2, tokens, deep), BF16),
            pltpu.VMEM((3, 2 * capacity, tokens), BF16),
            pltpu.VMEM((6, tokens, capacity), BF16),
            pltpu.VMEM((3, tokens, tokens), F32),
            pltpu.VMEM((capacity, deep), BF16),
            pltpu.VMEM((2, capacity, deep), BF16),
            pltpu.VMEM((ep, capacity, deep), BF16),
            pltpu.VMEM((ep * capacity, tp * units), BF16),
            pltpu.VMEM((2, 2, 3 * capacity, units), F32),
            pltpu.VMEM((tokens, deep), F32),
            pltpu.VMEM((capacity, deep), BF16),
            pltpu.VMEM((2, capacity, deep), BF16),
            pltpu.VMEM((2, capacity, deep), BF16),
            pltpu.VMEM((2, capacity, deep), BF16),
            pltpu.VMEM((2, tokens, deep), BF16),
            pltpu.VMEM((tokens, deep), BF16),
            pltpu.VMEM((4,) + gate.shape, BF16),
            pltpu.VMEM((4,) + up.shape, BF16),
            pltpu.VMEM((4,) + down.shape, BF16),
            dma((9,)),
            dma((3,)),
            dma(()),
            dma(()),
            dma((ep,)),
            dma((ep,)),
            dma((ep,)),
            dma(()),
            dma(()),
            dma(()),
            dma((2,)),
            dma(()),
            dma((2, parts)),
            dma((2,)),
            dma((2,)),
            dma((ep,)),
            dma((ep,)),
            dma(()),
            dma(()),
            dma((2,)),
            dma((2, fine)),
            dma((2,)),
            dma((fine,)),
            dma((tp,)),
            dma((tp,)),
            dma((3,)),
            dma((3,)),
            dma((3,)),
            dma((chunks,)),
            dma((3,)),
            dma((chunks,)),
            dma((2, 3)),
            dma((2, 2)),
            dma((fine,)),
        ],
        compiler_params=pltpu.CompilerParams(
            collective_id=0, has_side_effects=True, vmem_limit_bytes=60 * 2**20
        ),
    )(
        queries,
        keys,
        values,
        stop_bias.T,
        out_weight,
        mix_gain.reshape(1, deep),
        moe_input,
        ffn_gain.reshape(1, deep),
        expert_ids.T,
        expert_scores.T,
        gate,
        up,
        down,
    )
    results = [pltpu.with_memory_space_constraint(r, pltpu.VMEM) for r in results]
    return pl.pallas_call(
        settle_kernel,
        out_shape=tuple(jax.ShapeDtypeStruct(r.shape, r.dtype) for r in results),
        in_specs=[vmem] * 2,
        out_specs=(hbm, hbm),
        scratch_shapes=[dma((2,))],
    )(*results)


def pick_plan(groups, ep, tp, *args):
    heads = args[3].shape[1]
    width = args[0].shape[1] // ep
    head = args[0].shape[1] // heads
    exact = head & (head - 1) == 0 and head.bit_length() % 2 == 1
    if groups == 2 and tp == 4 and ep == 4 and heads % ep == 0 and width % 128 == 0 and exact:
        return fused_device(groups, ep, tp, *args)
    return per_device(*args)


def solution(mesh):
    return jax.shard_map(
        functools.partial(pick_plan, mesh.shape["grp"], mesh.shape["ep"], mesh.shape["tp"]),
        mesh=mesh,
        in_specs=(
            P(("grp", "ep"), "tp"),
            P(("grp", "ep"), "tp"),
            P(("grp", "ep"), "tp"),
            P(("grp", "ep"), "tp"),
            P("tp", None),
            P(),
            P(("grp", "ep", "tp"), None),
            P(),
            P(("grp", "ep", "tp"), None),
            P(("grp", "ep", "tp"), None),
            P("ep", None, "tp"),
            P("ep", None, "tp"),
            P("ep", "tp", None),
        ),
        out_specs=(P(("grp", "ep", "tp"), None), P(("grp", "ep", "tp"), None)),
        check_vma=False,
    )
```

```python
import functools

import jax
import jax.numpy as jnp
from jax import lax
from jax.experimental import pallas as pl
from jax.experimental.pallas import tpu as pltpu
from jax.sharding import PartitionSpec as P

MESH = pl.DeviceIdType.MESH
F32 = jnp.float32
BF16 = jnp.bfloat16


def norm_rows(values, gain):
    values = values.astype(jnp.float32)
    scale = lax.rsqrt(jnp.mean(values * values, axis=-1, keepdims=True) + 1e-06)
    return values * scale * gain


def break_terms(query_heads, query_place, key_block, bias_block, first):
    span = key_block.shape[0]
    heads = query_heads.shape[1]
    key_heads = key_block.reshape(span, heads, -1)
    scores = jnp.einsum("qhd,khd->hqk", query_heads, key_heads, preferred_element_type=jnp.float32)
    scores = scores * query_heads.shape[2] ** (-0.5) + bias_block.astype(jnp.float32).T[:, None, :]
    key_place = first + jnp.arange(span)
    past = (key_place[None, :] < query_place[:, None])[None]
    rest = jnp.where(past, jax.nn.log_sigmoid(-scores), 0.0)
    later = lax.cumsum(rest, axis=2, reverse=True)
    return (scores, past, rest, later)


def block_part(scores, past, rest, later, value_block, heads):
    within = later - rest
    local = jnp.where(past, jnp.exp(jax.nn.log_sigmoid(scores) + within), 0.0).astype(jnp.bfloat16)
    span = value_block.shape[0]
    value_heads = value_block.reshape(span, heads, -1)
    part = jnp.einsum("hqk,khd->qhd", local, value_heads, preferred_element_type=jnp.float32)
    return part.reshape(part.shape[0], -1)


def keep(state):
    return state


def dispatch_plan(normed, expert_ids, experts, capacity):
    rows, top = expert_ids.shape
    flat_ids = expert_ids.reshape(rows * top)
    onehot = (flat_ids[:, None] == jnp.arange(experts)[None, :]).astype(jnp.int32)
    earlier = jnp.cumsum(onehot, axis=0) - onehot
    place = jnp.sum(earlier * onehot, axis=1)
    target = flat_ids * capacity + place
    source = (
        jnp.zeros((experts * capacity,), jnp.int32)
        .at[target]
        .set(jnp.arange(rows * top, dtype=jnp.int32) // top + 1)
    )
    padded = jnp.concatenate([jnp.zeros((1, normed.shape[1]), normed.dtype), normed], axis=0)
    return (padded[source].reshape(experts, capacity, normed.shape[1]), target)


def expert_hidden(piece, gate_weight, up_weight):
    flat = piece.reshape(-1, piece.shape[-1])
    gate = jnp.dot(flat, gate_weight[0], preferred_element_type=jnp.float32)
    upward = jnp.dot(flat, up_weight[0], preferred_element_type=jnp.float32)
    hidden = (jax.nn.silu(gate) * upward).astype(jnp.bfloat16)
    return hidden.reshape(piece.shape[0], piece.shape[1], -1)


def send_back(summed):
    return lax.all_to_all(
        summed.astype(jnp.bfloat16), "ep", split_axis=0, concat_axis=0, tiled=True
    )


def return_rows(hidden_all, down_weight, sources):
    flat = hidden_all.reshape(-1, hidden_all.shape[2])
    product = jnp.dot(flat, down_weight[0], preferred_element_type=jnp.float32)
    return send_back(
        lax.psum_scatter(
            product.reshape(sources * lax.axis_size("tp"), hidden_all.shape[1], -1).astype(
                jnp.bfloat16
            ),
            "tp",
            scatter_dimension=0,
            tiled=True,
        ).astype(jnp.float32)
    )


def per_device(
    queries,
    keys,
    values,
    stop_bias,
    out_weight,
    mix_gain,
    moe_input,
    ffn_gain,
    expert_ids,
    expert_scores,
    gate_weight,
    up_weight,
    down_weight,
):
    span = queries.shape[0]
    heads = stop_bias.shape[1]
    width_heads = queries.shape[1]
    blocks = lax.axis_size("ep")
    own_first = lax.axis_index("ep") * span
    query_heads = queries.reshape(span, heads, -1)
    query_place = own_first + jnp.arange(span)

    def piece_rows(piece, index):
        return tuple((lax.dynamic_slice_in_dim(member, index * span, span, 0) for member in piece))

    start_state = (
        jnp.zeros((blocks, heads, span), jnp.float32),
        jnp.zeros((blocks, span, width_heads), jnp.float32),
    )
    piece = (
        lax.all_gather(keys, "ep", axis=0, tiled=True),
        lax.all_gather(values, "ep", axis=0, tiled=True),
        lax.all_gather(stop_bias, "ep", axis=0, tiled=True),
    )

    def one_block(index, state):
        key_block, value_block, bias_block = piece_rows(piece, index)
        first = index * span

        def compute(inner_state):
            totals, parts = inner_state
            scores, past, rest, later = break_terms(
                query_heads, query_place, key_block, bias_block, first
            )
            part = block_part(scores, past, rest, later, value_block, heads)
            number = first // span
            totals = lax.dynamic_update_index_in_dim(totals, later[:, :, 0], number, 0)
            parts = lax.dynamic_update_index_in_dim(parts, part, number, 0)
            return (totals, parts)

        return lax.cond(first <= own_first, compute, keep, state)

    totals, parts = lax.fori_loop(0, piece[0].shape[0] // span, one_block, start_state)
    carried = lax.cumsum(totals, axis=0, reverse=True) - totals
    factor = jnp.exp(carried).transpose(0, 2, 1)[:, :, :, None]
    attended = jnp.sum(factor * parts.reshape(blocks, span, heads, -1), axis=0).reshape(
        span, width_heads
    )
    attended = attended.astype(jnp.bfloat16)
    projected = lax.psum_scatter(
        jnp.dot(attended, out_weight, preferred_element_type=jnp.float32).astype(jnp.bfloat16),
        "tp",
        scatter_dimension=0,
        tiled=True,
    ).astype(jnp.float32)
    mixed = norm_rows(projected, mix_gain).astype(jnp.bfloat16)
    normed = norm_rows(moe_input, ffn_gain).astype(jnp.bfloat16)
    rows, top = expert_ids.shape
    experts = lax.axis_size("ep")
    capacity = 3 * rows * top // (2 * experts)
    weights = expert_scores / jnp.sum(expert_scores, axis=1, keepdims=True)
    outbound, target = dispatch_plan(normed, expert_ids, experts, capacity)
    arrived = lax.all_to_all(outbound, "ep", split_axis=0, concat_axis=0, tiled=True)
    hidden_all = expert_hidden(
        lax.all_gather(arrived, "tp", axis=0, tiled=True), gate_weight, up_weight
    )
    returned = return_rows(hidden_all, down_weight, arrived.shape[0])
    picked = returned.reshape(experts * capacity, -1)[target].reshape(rows, top, -1)
    experts_mixed = jnp.sum(picked.astype(jnp.float32) * weights[:, :, None], axis=1).astype(
        jnp.bfloat16
    )
    return (mixed, experts_mixed)


def layer_kernel(
    ep,
    capacity,
    head,
    q_ref,
    k_ref,
    v_ref,
    bias_ref,
    ow_ref,
    mix_gain_ref,
    x_ref,
    ffn_gain_ref,
    ids_ref,
    scores_ref,
    g_ref,
    u_ref,
    d_ref,
    mixed_ref,
    out_ref,
    x_own,
    gain_own,
    mix_own,
    ids_own,
    scores_own,
    qkv_all,
    bias_all,
    bias_rows,
    att_send,
    att_all,
    proj,
    proj_in,
    ow,
    meta,
    meta_in,
    normed_ref,
    dense_in,
    beside,
    beside_meta,
    sel,
    sel_back,
    gate_cols,
    outbound,
    relay_out,
    rows_in,
    hid,
    sofar,
    acc,
    back_out,
    back_in,
    outer_out,
    outer_in,
    dense_out,
    dense_back,
    g_all,
    u_all,
    d_all,
    load_sem,
    own_sem,
    ow_sem,
    pack_send,
    pack_recv,
    bias_send,
    bias_recv,
    row_send,
    row_recv,
    meta_send,
    meta_recv,
    dense_send,
    dense_recv,
    pass_send,
    beside_recv,
    beside_meta_send,
    beside_meta_recv,
    relay_send,
    relay_recv,
    att_ssem,
    att_rsem,
    back_ssem,
    back_rsem,
    outer_send,
    outer_recv,
    home_send,
    home_recv,
    proj_ssem,
    proj_rsem,
    near_send,
    near_recv,
    x_send,
    x_recv,
    y_send,
    y_recv,
    cross_send,
    cross_wide,
    cross_down,
):
    me = lax.axis_index("ep")
    tp = lax.axis_index("tp")
    grp = lax.axis_index("grp")
    chip, core = tp // 2, tp % 2
    mates = [None, chip * 2 + (1 - core), (1 - chip) * 2 + core, (1 - chip) * 2 + (1 - core)]
    span = q_ref.shape[0]
    width = qkv_all.shape[3]
    heads = width // head
    tokens, deep = x_ref.shape
    top = ids_ref.shape[0]
    parts = dense_recv.shape[1]
    fine = outer_recv.shape[1]
    wide_cuts = 2 * g_ref.shape[1]

    half = me // 2
    is_inner = lax.rem(me + 1, ep) // 2
    inner = is_inner == 1
    outside = is_inner == 0
    side = me + 1 - 2 * (me % 2)
    my_slot = 1 - is_inner
    far = (2 - half, 3 * (1 - half))

    loads = [
        pltpu.make_async_copy(s, t, load_sem.at[n])
        for n, (s, t) in enumerate(
            (
                (x_ref, x_own),
                (ids_ref, ids_own),
                (scores_ref, scores_own),
                (ffn_gain_ref, gain_own),
                (g_ref, g_all.at[0]),
                (u_ref, u_all.at[0]),
                (d_ref, d_all.at[0]),
                (mix_gain_ref, mix_own),
                (bias_ref, bias_all.at[me]),
            )
        )
    ]
    own = pl.ds(pl.multiple_of(me * width, width), width)
    mine = [
        pltpu.make_async_copy(r.at[:, own], qkv_all.at[me, n], own_sem.at[n])
        for n, r in enumerate((q_ref, k_ref, v_ref))
    ]
    ow_copy = pltpu.make_async_copy(ow_ref, ow, ow_sem)
    for copy in loads:
        copy.start()

    barrier = pltpu.get_barrier_semaphore()
    peers = [{"ep": lax.rem(me + r, ep)} for r in range(1, ep)]
    peers += [{"tp": mates[m]} for m in (1, 2, 3)] + [{"grp": 1 - grp}]
    for peer in peers:
        pl.semaphore_signal(barrier, inc=1, device_id=peer, device_id_type=MESH)
    for copy in mine:
        copy.start()
    ow_copy.start()

    def send(src, dst, ssem, rsem, peer):
        return pltpu.make_async_remote_copy(
            src_ref=src,
            dst_ref=dst,
            send_sem=ssem,
            recv_sem=rsem,
            device_id=peer,
            device_id_type=MESH,
        )

    mate = {"tp": mates[1]}

    def arrived(ref, sem):
        send(ref, ref, sem, sem, mate).wait_recv()

    def drained(ref, sem):
        send(ref, ref, sem, sem, mate).wait_send()

    def cols_of(c):
        return slice(c * (deep // parts), (c + 1) * (deep // parts))

    def strip(c):
        unit = deep // (2 * (fine - 1))
        edges = [0, 1] + [2 * n for n in range(1, fine)]
        return slice(edges[c] * unit, edges[c + 1] * unit)

    def piece_of(n, s, g):
        if n < wide_cuts:
            return (g_all, u_all)[n % 2].at[s, g, n // 2]
        return d_all.at[s, g, :, strip(n - wide_cuts)]

    def kind_of(n):
        return n % 2 if n < wide_cuts else 2

    chunks = wide_cuts + fine

    for n in range(4):
        loads[n].wait()
    gates = scores_own[...]
    gates = gates / jnp.sum(gates, axis=0, keepdims=True)
    meta[...] = jnp.zeros_like(meta)
    meta[0:top] = ids_own[...].astype(F32)
    meta[top : 2 * top] = gates
    values = x_own[...].astype(F32)
    scale = lax.rsqrt(jnp.mean(values * values, axis=-1, keepdims=True) + 1e-06)
    normed_ref[...] = (values * scale * gain_own[...]).astype(BF16)

    pl.semaphore_wait(barrier, len(peers))

    def over_x(n):
        return send(
            piece_of(n, 0, grp),
            piece_of(n, 2, grp),
            x_send,
            x_recv.at[n],
            {"tp": mates[2]},
        )

    loads[4].wait()
    over_x(0).start()
    send(meta, meta_in.at[my_slot], meta_send, meta_recv.at[my_slot], {"ep": far[0]}).start()

    def dense_of(slot, c):
        return send(
            normed_ref.at[:, cols_of(c)],
            dense_in.at[slot, :, cols_of(c)],
            dense_send,
            dense_recv.at[slot, c],
            {"ep": far[0]},
        )

    pieces = (q_ref, k_ref, v_ref)

    def pack(r, dest):
        cols = pl.ds(pl.multiple_of(dest * width, width), width)
        for n in range(3):
            send(
                pieces[n].at[:, cols],
                qkv_all.at[me, n],
                pack_send,
                pack_recv.at[me],
                {"ep": dest},
            ).start()
        send(bias_ref, bias_all.at[me], bias_send, bias_recv.at[me], {"ep": dest}).start()

    pack(0, far[0])
    pack(1, far[1])
    pack(2, side)

    @pl.when(inner)
    def _():
        for c in range(parts):
            dense_of(0, c).start()

    def beside_of(c):
        return send(
            normed_ref.at[:, cols_of(c)],
            beside.at[:, cols_of(c)],
            dense_send,
            beside_recv.at[c],
            {"ep": side},
        )

    beside_table = send(meta, beside_meta, beside_meta_send, beside_meta_recv, {"ep": side})

    @pl.when(outside)
    def _():
        beside_table.start()
        for c in range(parts):
            beside_of(c).start()

    loads[5].wait()
    for n in range(1, wide_cuts):
        over_x(n).start()
    loads[6].wait()
    for n in range(wide_cuts, chunks):
        over_x(n).start()
    nears = [
        send(r.at[0], r.at[1], near_send, near_recv.at[n], mate)
        for n, r in enumerate((g_all, u_all, d_all))
    ]
    square = (tokens, tokens)
    lane = lax.broadcasted_iota(jnp.int32, square, 1)
    sub = lax.broadcasted_iota(jnp.int32, square, 0)
    earlier = (sub < lane).astype(BF16)
    slots = lax.broadcasted_iota(jnp.int32, (capacity, tokens), 0).astype(F32)

    def route(table, at):
        named = jnp.zeros(square, F32)
        gate = jnp.zeros(square, F32)
        for n, e in enumerate((me, side)):
            place_of = e.astype(F32)
            for k in range(top):
                hit = table[k : k + 1, :] == place_of
                here = sub == n
                named = named + jnp.where(here & hit, 1.0, 0.0)
                gate = gate + jnp.where(here & hit, table[top + k : top + k + 1, :], 0.0)
        place = jnp.dot(named.astype(BF16), earlier, preferred_element_type=F32)
        for n in range(2):
            chosen = jnp.where(slots == place[n : n + 1, :], named[n : n + 1, :], 0.0)
            sel[at, n * capacity : (n + 1) * capacity] = chosen.astype(BF16)
            sel_back[2 * at + n] = chosen.T.astype(BF16)
        gate_cols[at] = gate.T

    def pick(at, block):
        return jnp.dot(sel[at], block, preferred_element_type=F32).astype(BF16)

    route(meta[...], 0)
    for c in range(parts):
        both = pick(0, normed_ref[:, cols_of(c)])
        rows_in[0, :, cols_of(c)] = both[:capacity]
        outbound[:, cols_of(c)] = both[capacity:]
    side_rows = send(outbound, rows_in.at[1], row_send, row_recv, {"ep": side})

    @pl.when(inner)
    def _():
        side_rows.start()

    def take(c):
        @pl.when(inner)
        def _():
            if c == 0:
                beside_table.wait_recv()
                route(beside_meta[...], 3)
            beside_of(c).wait_recv()
            send(
                beside.at[:, cols_of(c)],
                dense_in.at[1, :, cols_of(c)],
                pass_send,
                dense_recv.at[1, c],
                {"ep": far[0]},
            ).start()
            rows_in[1, :, cols_of(c)] = jnp.dot(
                sel[3, :capacity], beside[:, cols_of(c)], preferred_element_type=F32
            ).astype(BF16)

    def relay_of(slot, c):
        return send(
            relay_out.at[slot, :, cols_of(c)],
            rows_in.at[2 + slot, :, cols_of(c)],
            relay_send,
            relay_recv.at[slot],
            {"ep": side},
        )

    def relay(slot, c):
        @pl.when(inner)
        def _():
            if c == 0:
                arrived(meta_in.at[slot], meta_recv.at[slot])
                route(meta_in[slot], 1 + slot)
            dense_of(slot, c).wait_recv()
            both = pick(1 + slot, dense_in[slot, :, cols_of(c)])
            relay_out[slot, :, cols_of(c)] = both[capacity:]
            relay_of(slot, c).start()
            rows_in[2 + slot, :, cols_of(c)] = both[:capacity]

    def forward(n):
        over_x(n).wait_recv()
        send(
            piece_of(n, 2, grp),
            piece_of(n, 2, grp),
            y_send,
            y_recv.at[n],
            {"grp": 1 - grp},
        ).start()
        cross_of(0, n).start()

    def cross_of(way, n):
        g = grp if way == 0 else 1 - grp
        landed = cross_wide.at[way, n % 2] if n < wide_cuts else cross_down.at[n - wide_cuts]
        return send(piece_of(n, 2, g), piece_of(n, 3, g), cross_send, landed, mate)

    def forward_again(n):
        arrived(piece_of(n, 2, 1 - grp), y_recv.at[n])
        cross_of(1, n).start()

    units = hid.shape[1] // 4

    depth = deep // 2

    def rows_of(a, b):
        return slice(a * capacity, b * capacity)

    def activate(gate, up, s, rows):
        hid[rows, s * units : (s + 1) * units] = (gate / (1.0 + jnp.exp(-gate)) * up).astype(BF16)

    def hidden(s, a, b):
        flat = rows_in[a:b].reshape((b - a) * capacity, deep)
        gate = jnp.dot(flat, g_all[s].reshape(deep, units), preferred_element_type=F32)
        up = jnp.dot(flat, u_all[s].reshape(deep, units), preferred_element_type=F32)
        activate(gate, up, s, rows_of(a, b))

    def hidden_near(s):
        hidden(s, 0, 2)

    def hidden_first_slot(s):
        hidden(s, 2, 3)

    def hidden_late(s):
        hidden(s, 3, 4)

    def half_of(s, g):
        cols = pl.ds(pl.multiple_of(g * depth, depth), depth)
        flat = rows_in[0:3, :, cols].reshape(3 * capacity, depth)
        gate = jnp.dot(flat, g_all[s, g].reshape(depth, units), preferred_element_type=F32)
        up = jnp.dot(flat, u_all[s, g].reshape(depth, units), preferred_element_type=F32)
        return gate, up

    def hidden_first(s):
        gate, up = half_of(s, grp)
        sofar[s - 2, 0] = gate
        sofar[s - 2, 1] = up

    def hidden_second(s):
        gate, up = half_of(s, 1 - grp)
        activate(sofar[s - 2, 0] + gate, sofar[s - 2, 1] + up, s, rows_of(0, 3))

    block = (span, span)
    key_sub = lax.broadcasted_iota(jnp.int32, block, 0)
    key_lane = lax.broadcasted_iota(jnp.int32, block, 1)
    after = (key_sub > key_lane).astype(BF16)
    past = key_lane < key_sub

    def attend(i, heads_now):
        for h in heads_now:
            cols = slice(h * head, (h + 1) * head)
            query = qkv_all[i, 0][:, cols] * BF16(head**-0.5)
            for j in range(i, -1, -1):
                z = lax.dot_general(
                    query,
                    qkv_all[j, 1][:, cols],
                    (((1,), (1,)), ((), ())),
                    preferred_element_type=F32,
                )
                z = z + bias_rows[j, pl.ds(me * heads + h, 1), :]
                stop = jnp.minimum(z, 0.0) - jnp.log(1.0 + jnp.exp(jnp.minimum(z, -z)))
                rest = stop - z
                if j == i:
                    rest = jnp.where(past, rest, 0.0)
                hi = rest.astype(BF16)
                left = rest - hi.astype(F32)
                mid = left.astype(BF16)
                low = (left - mid.astype(F32)).astype(BF16)
                sums = jnp.dot(
                    jnp.concatenate([hi, mid, low], axis=0), after, preferred_element_type=F32
                )
                within = sums[:span] + sums[span : 2 * span] + sums[2 * span :]
                local = jnp.exp(stop + within)
                if j == i:
                    local = jnp.where(past, local, 0.0)
                part = jnp.dot(
                    local.astype(BF16), qkv_all[j, 2][:, cols], preferred_element_type=F32
                )
                total = part if j == i else total + jnp.exp(carry) * part
                if j > 0:
                    tally = jnp.sum(rest, axis=1, keepdims=True)
                    carry = tally if j == i else carry + tally
            att_send[i, :, cols] = total.astype(BF16)
        if heads_now[-1] != heads - 1:
            return

        @pl.when(me == i)
        def _():
            att_all[i] = att_send[i]

        @pl.when(me != i)
        def _():
            att_of(i, me).start()

    def att_of(i, j):
        return send(att_send.at[i], att_all.at[j], att_ssem, att_rsem.at[j], {"ep": i})

    def packs_here():
        for copy in mine:
            copy.wait()
        loads[8].wait()
        for r in range(1, ep):
            source = lax.rem(me + r, ep)
            arrived(qkv_all.at[source], pack_recv.at[source])
            arrived(bias_all.at[source], bias_recv.at[source])
        bias_rows[...] = bias_all[...].astype(F32)

    firsts, lasts = tuple(range(heads // 2)), tuple(range(heads // 2, heads))
    everyone = firsts + lasts
    W = wide_cuts
    lag = 3
    near_at = (2, 4, 10)
    for n in range(W):
        forward(n)
        if n >= lag:
            forward_again(n - lag)
        if n in (7, 9, 11, 13):
            relay(0, (n - 7) // 2)
        if n in near_at:
            nears[near_at.index(n)].start()
        if n == 5:
            packs_here()
            attend(3, firsts)
        if n == 6:
            attend(3, lasts)
        if n == 7:
            attend(0, everyone)
        if n == 8:
            attend(2, everyone)
        if n == 9:
            attend(1, everyone)
        if n == 10:
            take(0)
            take(1)
        if n == 12:
            take(2)
        if n == 14:
            take(3)

            @pl.when(outside)
            def _():
                side_rows.wait_recv()

            hidden_near(0)
        if n == 15:
            for copy in nears:
                copy.wait_recv()
            hidden_near(1)

    forward_again(W - 3)
    forward(W)
    forward(W + 1)

    @pl.when(outside)
    def _():
        arrived(relay_out.at[0], relay_recv.at[0])

    hidden_first_slot(0)
    forward_again(W - 2)
    hidden_first_slot(1)
    relay(1, 0)
    forward(W + 2)
    for n, r in enumerate((g_all, u_all)):
        arrived(r.at[3, grp], cross_wide.at[0, n])
    hidden_first(2)
    hidden_first(3)
    forward(W + 3)
    forward_again(W - 1)
    hidden_second(2)
    forward_again(W)
    relay(1, 1)
    forward(W + 4)
    for n, r in enumerate((g_all, u_all)):
        arrived(r.at[3, 1 - grp], cross_wide.at[1, n])
    hidden_second(3)
    forward_again(W + 1)

    def outer_of(slot, c):
        cols = strip(c)
        return send(
            outer_out.at[slot, :, cols],
            outer_in.at[slot, :, cols],
            outer_send,
            outer_recv.at[slot, c],
            {"ep": side},
        )

    thirds = [
        slice(strip(a).start, strip(b).stop) for a, b in ((0, 3), (4, fine - 3), (fine - 2, fine - 1))
    ]

    def back_of(cols):
        return send(
            back_out.at[:, cols],
            back_in.at[1, :, cols],
            back_ssem,
            back_rsem.at[sum(cols.start >= e.start for e in thirds[1:])],
            {"ep": side},
        )

    def lower(cols, a, b):
        down = jnp.concatenate(
            [d_all[s, :, :, cols].reshape(units, -1) for s in range(4)], axis=0
        )
        return jnp.dot(hid[rows_of(a, b)], down, preferred_element_type=F32).astype(BF16)

    def put_far(slot, c, rows):
        outer_out[slot, :, strip(c)] = rows

        @pl.when(outside)
        def _():
            outer_of(slot, c).start()

    held = 3

    def final(c):
        cols = strip(c)
        arrived(d_all.at[3, :, :, cols], cross_down.at[c])
        rows = lower(cols, 0, 3)
        put_far(0, c, rows[rows_of(2, 3)])
        back_in[0, :, cols] = rows[rows_of(0, 1)]
        back_out[:, cols] = rows[rows_of(1, 2)]

        if c > held:

            @pl.when(inner)
            def _():
                back_of(cols).start()

    def final_late(c):
        put_far(1, c, lower(strip(c), 3, 4))

    def back_strips(first, last):
        @pl.when(outside)
        def _():
            back_of(slice(strip(first).start, strip(last).stop)).start()

    def home_of(slot, c):
        return send(
            dense_out.at[slot, :, strip(c)],
            dense_back.at[:, strip(c)],
            home_send,
            home_recv.at[c // (fine - 1)],
            {"ep": far[slot]},
        )

    def weigh(at, near_rows, far_rows):
        gate = gate_cols[at]
        here = jnp.dot(sel_back[2 * at], near_rows, preferred_element_type=F32)
        there = jnp.dot(sel_back[2 * at + 1], far_rows, preferred_element_type=F32)
        return gate[:, 0:1] * here + gate[:, 1:2] * there

    def return_home(slot, c):
        cols = strip(c)

        @pl.when(inner)
        def _():
            outer_of(slot, c).wait_recv()
            dense_out[slot, :, cols] = weigh(
                1 + slot, outer_out[slot, :, cols], outer_in[slot, :, cols]
            ).astype(BF16)
            home_of(slot, c).start()

    final(0)
    forward(W + 5)
    forward_again(W + 2)
    final(1)
    forward(W + 6)
    forward_again(W + 3)
    relay(1, 2)
    final(2)
    return_home(0, 0)
    relay(1, 3)
    return_home(0, 1)
    forward(W + 7)
    forward_again(W + 4)
    final(3)
    return_home(0, 2)

    @pl.when(inner)
    def _():
        back_of(slice(0, strip(held).stop)).start()

    forward(W + 8)
    forward_again(W + 5)
    final(4)
    back_strips(0, 1)
    return_home(0, 3)
    forward_again(W + 6)
    final(5)
    return_home(0, 4)
    forward_again(W + 7)
    final(6)
    return_home(0, 5)

    @pl.when(outside)
    def _():
        arrived(relay_out.at[1], relay_recv.at[1])

    hidden_late(0)
    hidden_late(1)
    forward_again(W + 8)
    final(7)
    return_home(0, 6)
    hidden_late(2)
    hidden_late(3)
    final(8)
    return_home(0, 7)
    return_home(0, 8)
    final_late(0)
    final_late(1)
    final_late(2)
    final_late(3)
    return_home(1, 0)
    return_home(1, 1)
    for c in range(4, fine):
        final_late(c)
    back_strips(2, 3)
    back_strips(4, fine - 3)
    back_strips(fine - 2, fine - 1)
    return_home(1, 2)
    for j in range(ep):

        @pl.when(me != j)
        def _():
            arrived(att_all.at[j], att_rsem.at[j])

    ow_copy.wait()
    attended = jnp.concatenate([att_all[j] for j in range(ep)], axis=1)
    term = jnp.dot(attended, ow[...], preferred_element_type=F32).astype(BF16)
    proj[...] = term.reshape(proj.shape)
    shares = [
        send(proj.at[mates[m]], proj_in.at[m], proj_ssem.at[m], proj_rsem.at[m], {"tp": mates[m]})
        for m in (2, 3, 1)
    ]
    for copy in shares:
        copy.start()
    for c in range(3, fine):
        return_home(1, c)
    whole = proj[tp].astype(F32)
    for copy in shares:
        copy.wait_recv()
    for m in (1, 2, 3):
        whole = whole + proj_in[m].astype(F32)
    loads[7].wait()
    scale = lax.rsqrt(jnp.mean(whole * whole, axis=-1, keepdims=True) + 1e-06)
    mixed_ref[...] = (whole * scale * mix_own[...]).astype(BF16)
    drained(normed_ref, dense_send)
    drained(g_all.at[pl.ds(0, 3), 0], x_send)
    drained(g_all.at[pl.ds(0, 3), 0], y_send)
    drained(g_all.at[pl.ds(0, 3)], cross_send)
    drained(g_all.at[pl.ds(0, 3)], near_send)
    drained(qkv_all.at[pl.ds(0, 3)], pack_send)
    drained(bias_all.at[pl.ds(0, ep - 1)], bias_send)

    @pl.when(inner)
    def _():
        side_rows.wait_send()
        drained(beside, pass_send)

    @pl.when(outside)
    def _():
        beside_table.wait_send()

    drained(meta, meta_send)
    drained(att_send.at[pl.ds(0, ep - 1)], att_ssem)

    for copy in shares:
        copy.wait_send()
    for n, cols in enumerate(thirds):
        arrived(back_in.at[1, :, cols], back_rsem.at[n])
        acc[:, cols] = weigh(0, back_in[0, :, cols], back_in[1, :, cols])
    drained(back_out, back_ssem)

    @pl.when(outside)
    def _():
        drained(outer_out, outer_send)

    for n, cols in enumerate((slice(0, strip(fine - 1).start), strip(fine - 1))):
        arrived(dense_back.at[:, cols], home_recv.at[n])
        out_ref[:, cols] = (acc[:, cols] + dense_back[:, cols].astype(F32)).astype(BF16)

    @pl.when(inner)
    def _():
        drained(relay_out, relay_send)
        drained(dense_out, home_send)


def settle_kernel(mixed_ref, out_ref, mixed_to, out_to, sems):
    copies = [
        pltpu.make_async_copy(out_ref, out_to, sems.at[0]),
        pltpu.make_async_copy(mixed_ref, mixed_to, sems.at[1]),
    ]
    for copy in copies:
        copy.start()
    for copy in copies:
        copy.wait()


def fused_device(
    groups,
    ep,
    tp,
    queries,
    keys,
    values,
    stop_bias,
    out_weight,
    mix_gain,
    moe_input,
    ffn_gain,
    expert_ids,
    expert_scores,
    gate_weight,
    up_weight,
    down_weight,
):
    span, cols = queries.shape
    tokens, deep = moe_input.shape
    top = expert_ids.shape[1]
    capacity = 3 * tokens * top // (2 * ep)
    width = cols // ep
    heads = stop_bias.shape[1]
    units = gate_weight.shape[2]
    cuts = 8
    parts = 4
    fine = 9
    lines = 8
    gate = gate_weight.reshape(groups, cuts, deep // (groups * cuts), units)
    up = up_weight.reshape(gate.shape)
    down = down_weight.reshape(groups, units // groups, deep)
    chunks = 2 * cuts + fine
    vmem = pl.BlockSpec(memory_space=pltpu.VMEM)
    hbm = pl.BlockSpec(memory_space=pl.ANY)
    dma = pltpu.SemaphoreType.DMA
    results = pl.pallas_call(
        functools.partial(layer_kernel, ep, capacity, cols // heads),
        out_shape=(
            pltpu.VMEM((span // tp, deep), BF16),
            pltpu.VMEM((tokens, deep), BF16),
        ),
        in_specs=[hbm] * 13,
        out_specs=(vmem, vmem),
        scratch_shapes=[
            pltpu.VMEM((tokens, deep), BF16),
            pltpu.VMEM((1, deep), F32),
            pltpu.VMEM((1, deep), F32),
            pltpu.VMEM((top, tokens), jnp.int32),
            pltpu.VMEM((top, tokens), F32),
            pltpu.VMEM((ep, 3, span, width), BF16),
            pltpu.VMEM((ep, heads, span), BF16),
            pltpu.VMEM((ep, heads, span), F32),
            pltpu.VMEM((ep, span, width), BF16),
            pltpu.VMEM((ep, span, width), BF16),
            pltpu.VMEM((tp, span // tp, deep), BF16),
            pltpu.VMEM((tp, span // tp, deep), BF16),
            pltpu.VMEM(out_weight.shape, BF16),
            pltpu.VMEM((lines, tokens), F32),
            pltpu.VMEM((2, lines, tokens), F32),
            pltpu.VMEM((tokens, deep), BF16),
            pltpu.VMEM((2, tokens, deep), BF16),
            pltpu.VMEM((tokens, deep), BF16),
            pltpu.VMEM((lines, tokens), F32),
            pltpu.VMEM((4, 2 * capacity, tokens), BF16),
            pltpu.VMEM((8, tokens, capacity), BF16),
            pltpu.VMEM((4, tokens, tokens), F32),
            pltpu.VMEM((capacity, deep), BF16),
            pltpu.VMEM((2, capacity, deep), BF16),
            pltpu.VMEM((ep, capacity, deep), BF16),
            pltpu.VMEM((ep * capacity, tp * units), BF16),
            pltpu.VMEM((2, 2, 3 * capacity, units), F32),
            pltpu.VMEM((tokens, deep), F32),
            pltpu.VMEM((capacity, deep), BF16),
            pltpu.VMEM((2, capacity, deep), BF16),
            pltpu.VMEM((2, capacity, deep), BF16),
            pltpu.VMEM((2, capacity, deep), BF16),
            pltpu.VMEM((2, tokens, deep), BF16),
            pltpu.VMEM((tokens, deep), BF16),
            pltpu.VMEM((4,) + gate.shape, BF16),
            pltpu.VMEM((4,) + up.shape, BF16),
            pltpu.VMEM((4,) + down.shape, BF16),
            dma((9,)),
            dma((3,)),
            dma(()),
            dma(()),
            dma((ep,)),
            dma(()),
            dma((ep,)),
            dma(()),
            dma(()),
            dma(()),
            dma((2,)),
            dma(()),
            dma((2, parts)),
            dma(()),
            dma((parts,)),
            dma(()),
            dma(()),
            dma(()),
            dma((2,)),
            dma(()),
            dma((ep,)),
            dma(()),
            dma((3,)),
            dma(()),
            dma((2, fine)),
            dma(()),
            dma((2,)),
            dma((tp,)),
            dma((tp,)),
            dma(()),
            dma((3,)),
            dma(()),
            dma((chunks,)),
            dma(()),
            dma((chunks,)),
            dma(()),
            dma((2, 2)),
            dma((fine,)),
        ],
        compiler_params=pltpu.CompilerParams(
            collective_id=0, has_side_effects=True, vmem_limit_bytes=60 * 2**20
        ),
    )(
        queries,
        keys,
        values,
        stop_bias.T,
        out_weight,
        mix_gain.reshape(1, deep),
        moe_input,
        ffn_gain.reshape(1, deep),
        expert_ids.T,
        expert_scores.T,
        gate,
        up,
        down,
    )
    results = [pltpu.with_memory_space_constraint(r, pltpu.VMEM) for r in results]
    return pl.pallas_call(
        settle_kernel,
        out_shape=tuple(jax.ShapeDtypeStruct(r.shape, r.dtype) for r in results),
        in_specs=[vmem] * 2,
        out_specs=(hbm, hbm),
        scratch_shapes=[dma((2,))],
    )(*results)


def pick_plan(groups, ep, tp, *args):
    heads = args[3].shape[1]
    width = args[0].shape[1] // ep
    head = args[0].shape[1] // heads
    exact = head & (head - 1) == 0 and head.bit_length() % 2 == 1
    if groups == 2 and tp == 4 and ep == 4 and heads % ep == 0 and width % 128 == 0 and exact:
        return fused_device(groups, ep, tp, *args)
    return per_device(*args)


def solution(mesh):
    return jax.shard_map(
        functools.partial(pick_plan, mesh.shape["grp"], mesh.shape["ep"], mesh.shape["tp"]),
        mesh=mesh,
        in_specs=(
            P(("grp", "ep"), "tp"),
            P(("grp", "ep"), "tp"),
            P(("grp", "ep"), "tp"),
            P(("grp", "ep"), "tp"),
            P("tp", None),
            P(),
            P(("grp", "ep", "tp"), None),
            P(),
            P(("grp", "ep", "tp"), None),
            P(("grp", "ep", "tp"), None),
            P("ep", None, "tp"),
            P("ep", None, "tp"),
            P("ep", "tp", None),
        ),
        out_specs=(P(("grp", "ep", "tp"), None), P(("grp", "ep", "tp"), None)),
        check_vma=False,
    )
```

```python
import functools

import jax
import jax.numpy as jnp
from jax import lax
from jax.experimental import pallas as pl
from jax.experimental.pallas import tpu as pltpu
from jax.sharding import PartitionSpec as P

MESH = pl.DeviceIdType.MESH
F32 = jnp.float32
BF16 = jnp.bfloat16


def norm_rows(values, gain):
    values = values.astype(jnp.float32)
    scale = lax.rsqrt(jnp.mean(values * values, axis=-1, keepdims=True) + 1e-06)
    return values * scale * gain


def break_terms(query_heads, query_place, key_block, bias_block, first):
    span = key_block.shape[0]
    heads = query_heads.shape[1]
    key_heads = key_block.reshape(span, heads, -1)
    scores = jnp.einsum("qhd,khd->hqk", query_heads, key_heads, preferred_element_type=jnp.float32)
    scores = scores * query_heads.shape[2] ** (-0.5) + bias_block.astype(jnp.float32).T[:, None, :]
    key_place = first + jnp.arange(span)
    past = (key_place[None, :] < query_place[:, None])[None]
    rest = jnp.where(past, jax.nn.log_sigmoid(-scores), 0.0)
    later = lax.cumsum(rest, axis=2, reverse=True)
    return (scores, past, rest, later)


def block_part(scores, past, rest, later, value_block, heads):
    within = later - rest
    local = jnp.where(past, jnp.exp(jax.nn.log_sigmoid(scores) + within), 0.0).astype(jnp.bfloat16)
    span = value_block.shape[0]
    value_heads = value_block.reshape(span, heads, -1)
    part = jnp.einsum("hqk,khd->qhd", local, value_heads, preferred_element_type=jnp.float32)
    return part.reshape(part.shape[0], -1)


def keep(state):
    return state


def dispatch_plan(normed, expert_ids, experts, capacity):
    rows, top = expert_ids.shape
    flat_ids = expert_ids.reshape(rows * top)
    onehot = (flat_ids[:, None] == jnp.arange(experts)[None, :]).astype(jnp.int32)
    earlier = jnp.cumsum(onehot, axis=0) - onehot
    place = jnp.sum(earlier * onehot, axis=1)
    target = flat_ids * capacity + place
    source = (
        jnp.zeros((experts * capacity,), jnp.int32)
        .at[target]
        .set(jnp.arange(rows * top, dtype=jnp.int32) // top + 1)
    )
    padded = jnp.concatenate([jnp.zeros((1, normed.shape[1]), normed.dtype), normed], axis=0)
    return (padded[source].reshape(experts, capacity, normed.shape[1]), target)


def expert_hidden(piece, gate_weight, up_weight):
    flat = piece.reshape(-1, piece.shape[-1])
    gate = jnp.dot(flat, gate_weight[0], preferred_element_type=jnp.float32)
    upward = jnp.dot(flat, up_weight[0], preferred_element_type=jnp.float32)
    hidden = (jax.nn.silu(gate) * upward).astype(jnp.bfloat16)
    return hidden.reshape(piece.shape[0], piece.shape[1], -1)


def send_back(summed):
    return lax.all_to_all(
        summed.astype(jnp.bfloat16), "ep", split_axis=0, concat_axis=0, tiled=True
    )


def return_rows(hidden_all, down_weight, sources):
    flat = hidden_all.reshape(-1, hidden_all.shape[2])
    product = jnp.dot(flat, down_weight[0], preferred_element_type=jnp.float32)
    return send_back(
        lax.psum_scatter(
            product.reshape(sources * lax.axis_size("tp"), hidden_all.shape[1], -1).astype(
                jnp.bfloat16
            ),
            "tp",
            scatter_dimension=0,
            tiled=True,
        ).astype(jnp.float32)
    )


def per_device(
    queries,
    keys,
    values,
    stop_bias,
    out_weight,
    mix_gain,
    moe_input,
    ffn_gain,
    expert_ids,
    expert_scores,
    gate_weight,
    up_weight,
    down_weight,
):
    span = queries.shape[0]
    heads = stop_bias.shape[1]
    width_heads = queries.shape[1]
    blocks = lax.axis_size("ep")
    own_first = lax.axis_index("ep") * span
    query_heads = queries.reshape(span, heads, -1)
    query_place = own_first + jnp.arange(span)

    def piece_rows(piece, index):
        return tuple((lax.dynamic_slice_in_dim(member, index * span, span, 0) for member in piece))

    start_state = (
        jnp.zeros((blocks, heads, span), jnp.float32),
        jnp.zeros((blocks, span, width_heads), jnp.float32),
    )
    piece = (
        lax.all_gather(keys, "ep", axis=0, tiled=True),
        lax.all_gather(values, "ep", axis=0, tiled=True),
        lax.all_gather(stop_bias, "ep", axis=0, tiled=True),
    )

    def one_block(index, state):
        key_block, value_block, bias_block = piece_rows(piece, index)
        first = index * span

        def compute(inner_state):
            totals, parts = inner_state
            scores, past, rest, later = break_terms(
                query_heads, query_place, key_block, bias_block, first
            )
            part = block_part(scores, past, rest, later, value_block, heads)
            number = first // span
            totals = lax.dynamic_update_index_in_dim(totals, later[:, :, 0], number, 0)
            parts = lax.dynamic_update_index_in_dim(parts, part, number, 0)
            return (totals, parts)

        return lax.cond(first <= own_first, compute, keep, state)

    totals, parts = lax.fori_loop(0, piece[0].shape[0] // span, one_block, start_state)
    carried = lax.cumsum(totals, axis=0, reverse=True) - totals
    factor = jnp.exp(carried).transpose(0, 2, 1)[:, :, :, None]
    attended = jnp.sum(factor * parts.reshape(blocks, span, heads, -1), axis=0).reshape(
        span, width_heads
    )
    attended = attended.astype(jnp.bfloat16)
    projected = lax.psum_scatter(
        jnp.dot(attended, out_weight, preferred_element_type=jnp.float32).astype(jnp.bfloat16),
        "tp",
        scatter_dimension=0,
        tiled=True,
    ).astype(jnp.float32)
    mixed = norm_rows(projected, mix_gain).astype(jnp.bfloat16)
    normed = norm_rows(moe_input, ffn_gain).astype(jnp.bfloat16)
    rows, top = expert_ids.shape
    experts = lax.axis_size("ep")
    capacity = 3 * rows * top // (2 * experts)
    weights = expert_scores / jnp.sum(expert_scores, axis=1, keepdims=True)
    outbound, target = dispatch_plan(normed, expert_ids, experts, capacity)
    arrived = lax.all_to_all(outbound, "ep", split_axis=0, concat_axis=0, tiled=True)
    hidden_all = expert_hidden(
        lax.all_gather(arrived, "tp", axis=0, tiled=True), gate_weight, up_weight
    )
    returned = return_rows(hidden_all, down_weight, arrived.shape[0])
    picked = returned.reshape(experts * capacity, -1)[target].reshape(rows, top, -1)
    experts_mixed = jnp.sum(picked.astype(jnp.float32) * weights[:, :, None], axis=1).astype(
        jnp.bfloat16
    )
    return (mixed, experts_mixed)


def layer_kernel(
    ep,
    capacity,
    head,
    q_ref,
    k_ref,
    v_ref,
    bias_ref,
    ow_ref,
    mix_gain_ref,
    x_ref,
    ffn_gain_ref,
    ids_ref,
    scores_ref,
    g_ref,
    u_ref,
    d_ref,
    mixed_ref,
    out_ref,
    x_own,
    gain_own,
    mix_own,
    ids_own,
    scores_own,
    qkv_all,
    bias_all,
    bias_rows,
    att_send,
    att_all,
    proj,
    proj_in,
    ow,
    meta,
    meta_in,
    normed_ref,
    dense_in,
    beside,
    beside_meta,
    sel,
    sel_back,
    gate_cols,
    outbound,
    relay_out,
    rows_in,
    hid,
    sofar,
    acc,
    back_out,
    back_in,
    outer_out,
    outer_in,
    dense_out,
    dense_back,
    g_all,
    u_all,
    d_all,
    load_sem,
    own_sem,
    ow_sem,
    pack_send,
    pack_recv,
    bias_send,
    bias_recv,
    row_send,
    row_recv,
    meta_send,
    meta_recv,
    dense_send,
    dense_recv,
    pass_send,
    beside_recv,
    beside_meta_send,
    beside_meta_recv,
    relay_send,
    relay_recv,
    att_ssem,
    att_rsem,
    back_ssem,
    back_rsem,
    outer_send,
    outer_recv,
    home_send,
    home_recv,
    proj_ssem,
    proj_rsem,
    near_send,
    near_recv,
    x_send,
    x_recv,
    y_send,
    y_recv,
    cross_send,
    cross_wide,
    cross_down,
):
    me = lax.axis_index("ep")
    tp = lax.axis_index("tp")
    grp = lax.axis_index("grp")
    chip, core = tp // 2, tp % 2
    mates = [None, chip * 2 + (1 - core), (1 - chip) * 2 + core, (1 - chip) * 2 + (1 - core)]
    span = q_ref.shape[0]
    width = qkv_all.shape[3]
    heads = width // head
    tokens, deep = x_ref.shape
    top = ids_ref.shape[0]
    parts = dense_recv.shape[1]
    fine = outer_recv.shape[1]
    wide_cuts = 2 * g_ref.shape[1]

    half = me // 2
    is_inner = lax.rem(me + 1, ep) // 2
    inner = is_inner == 1
    outside = is_inner == 0
    side = me + 1 - 2 * (me % 2)
    my_slot = 1 - is_inner
    far = (2 - half, 3 * (1 - half))

    loads = [
        pltpu.make_async_copy(s, t, load_sem.at[n])
        for n, (s, t) in enumerate(
            (
                (x_ref, x_own),
                (ids_ref, ids_own),
                (scores_ref, scores_own),
                (ffn_gain_ref, gain_own),
                (g_ref, g_all.at[0]),
                (u_ref, u_all.at[0]),
                (d_ref, d_all.at[0]),
                (mix_gain_ref, mix_own),
                (bias_ref, bias_all.at[me]),
            )
        )
    ]
    own = pl.ds(pl.multiple_of(me * width, width), width)
    mine = [
        pltpu.make_async_copy(r.at[:, own], qkv_all.at[me, n], own_sem.at[n])
        for n, r in enumerate((q_ref, k_ref, v_ref))
    ]
    ow_copy = pltpu.make_async_copy(ow_ref, ow, ow_sem)
    for copy in loads:
        copy.start()

    barrier = pltpu.get_barrier_semaphore()
    peers = [{"ep": lax.rem(me + r, ep)} for r in range(1, ep)]
    peers += [{"tp": mates[m]} for m in (1, 2, 3)] + [{"grp": 1 - grp}]
    for peer in peers:
        pl.semaphore_signal(barrier, inc=1, device_id=peer, device_id_type=MESH)
    for copy in mine:
        copy.start()
    ow_copy.start()

    def send(src, dst, ssem, rsem, peer):
        return pltpu.make_async_remote_copy(
            src_ref=src,
            dst_ref=dst,
            send_sem=ssem,
            recv_sem=rsem,
            device_id=peer,
            device_id_type=MESH,
        )

    mate = {"tp": mates[1]}

    def arrived(ref, sem):
        send(ref, ref, sem, sem, mate).wait_recv()

    def drained(ref, sem):
        send(ref, ref, sem, sem, mate).wait_send()

    def cols_of(c):
        return slice(c * (deep // parts), (c + 1) * (deep // parts))

    def strip(c):
        unit = deep // (2 * (fine - 1))
        edges = [0, 1] + [2 * n for n in range(1, fine)]
        return slice(edges[c] * unit, edges[c + 1] * unit)

    def piece_of(n, s, g):
        if n < wide_cuts:
            return (g_all, u_all)[n % 2].at[s, g, n // 2]
        return d_all.at[s, g, :, strip(n - wide_cuts)]

    def kind_of(n):
        return n % 2 if n < wide_cuts else 2

    chunks = wide_cuts + fine

    for n in range(4):
        loads[n].wait()
    gates = scores_own[...]
    gates = gates / jnp.sum(gates, axis=0, keepdims=True)
    meta[...] = jnp.zeros_like(meta)
    meta[0:top] = ids_own[...].astype(F32)
    meta[top : 2 * top] = gates
    values = x_own[...].astype(F32)
    scale = lax.rsqrt(jnp.mean(values * values, axis=-1, keepdims=True) + 1e-06)
    normed_ref[...] = (values * scale * gain_own[...]).astype(BF16)

    pl.semaphore_wait(barrier, len(peers))

    def over_x(n):
        return send(
            piece_of(n, 0, grp),
            piece_of(n, 2, grp),
            x_send,
            x_recv.at[n],
            {"tp": mates[2]},
        )

    loads[4].wait()
    over_x(0).start()
    send(meta, meta_in.at[my_slot], meta_send, meta_recv.at[my_slot], {"ep": far[0]}).start()

    def dense_of(slot, c):
        return send(
            normed_ref.at[:, cols_of(c)],
            dense_in.at[slot, :, cols_of(c)],
            dense_send,
            dense_recv.at[slot, c],
            {"ep": far[0]},
        )

    pieces = (q_ref, k_ref, v_ref)

    def pack(r, dest):
        cols = pl.ds(pl.multiple_of(dest * width, width), width)
        for n in range(3):
            send(
                pieces[n].at[:, cols],
                qkv_all.at[me, n],
                pack_send,
                pack_recv.at[me],
                {"ep": dest},
            ).start()
        send(bias_ref, bias_all.at[me], bias_send, bias_recv.at[me], {"ep": dest}).start()

    pack(0, far[0])
    pack(1, far[1])
    pack(2, side)

    @pl.when(inner)
    def _():
        for c in range(parts):
            dense_of(0, c).start()

    def beside_of(c):
        return send(
            normed_ref.at[:, cols_of(c)],
            beside.at[:, cols_of(c)],
            dense_send,
            beside_recv.at[c],
            {"ep": side},
        )

    beside_table = send(meta, beside_meta, beside_meta_send, beside_meta_recv, {"ep": side})

    @pl.when(outside)
    def _():
        beside_table.start()
        for c in range(parts):
            beside_of(c).start()

    loads[5].wait()
    for n in range(1, wide_cuts):
        over_x(n).start()
    loads[6].wait()
    for n in range(wide_cuts, chunks):
        over_x(n).start()
    nears = [
        send(r.at[0], r.at[1], near_send, near_recv.at[n], mate)
        for n, r in enumerate((g_all, u_all, d_all))
    ]
    square = (tokens, tokens)
    lane = lax.broadcasted_iota(jnp.int32, square, 1)
    sub = lax.broadcasted_iota(jnp.int32, square, 0)
    earlier = (sub < lane).astype(BF16)
    slots = lax.broadcasted_iota(jnp.int32, (capacity, tokens), 0).astype(F32)

    def route(table, at):
        named = jnp.zeros(square, F32)
        gate = jnp.zeros(square, F32)
        for n, e in enumerate((me, side)):
            place_of = e.astype(F32)
            for k in range(top):
                hit = table[k : k + 1, :] == place_of
                here = sub == n
                named = named + jnp.where(here & hit, 1.0, 0.0)
                gate = gate + jnp.where(here & hit, table[top + k : top + k + 1, :], 0.0)
        place = jnp.dot(named.astype(BF16), earlier, preferred_element_type=F32)
        for n in range(2):
            chosen = jnp.where(slots == place[n : n + 1, :], named[n : n + 1, :], 0.0)
            sel[at, n * capacity : (n + 1) * capacity] = chosen.astype(BF16)
            sel_back[2 * at + n] = chosen.T.astype(BF16)
        gate_cols[at] = gate.T

    def pick(at, block):
        return jnp.dot(sel[at], block, preferred_element_type=F32).astype(BF16)

    route(meta[...], 0)
    for c in range(parts):
        both = pick(0, normed_ref[:, cols_of(c)])
        rows_in[0, :, cols_of(c)] = both[:capacity]
        outbound[:, cols_of(c)] = both[capacity:]
    side_rows = send(outbound, rows_in.at[1], row_send, row_recv, {"ep": side})

    @pl.when(inner)
    def _():
        side_rows.start()

    def take(c):
        @pl.when(inner)
        def _():
            if c == 0:
                beside_table.wait_recv()
                route(beside_meta[...], 3)
            beside_of(c).wait_recv()
            send(
                beside.at[:, cols_of(c)],
                dense_in.at[1, :, cols_of(c)],
                pass_send,
                dense_recv.at[1, c],
                {"ep": far[0]},
            ).start()
            rows_in[1, :, cols_of(c)] = jnp.dot(
                sel[3, :capacity], beside[:, cols_of(c)], preferred_element_type=F32
            ).astype(BF16)

    def relay_of(slot, c):
        return send(
            relay_out.at[slot, :, cols_of(c)],
            rows_in.at[2 + slot, :, cols_of(c)],
            relay_send,
            relay_recv.at[slot],
            {"ep": side},
        )

    def relay(slot, c):
        @pl.when(inner)
        def _():
            if c == 0:
                arrived(meta_in.at[slot], meta_recv.at[slot])
                route(meta_in[slot], 1 + slot)
            dense_of(slot, c).wait_recv()
            both = pick(1 + slot, dense_in[slot, :, cols_of(c)])
            relay_out[slot, :, cols_of(c)] = both[capacity:]
            relay_of(slot, c).start()
            rows_in[2 + slot, :, cols_of(c)] = both[:capacity]

    def forward(n):
        over_x(n).wait_recv()
        send(
            piece_of(n, 2, grp),
            piece_of(n, 2, grp),
            y_send,
            y_recv.at[n],
            {"grp": 1 - grp},
        ).start()
        cross_of(0, n).start()

    def cross_of(way, n):
        g = grp if way == 0 else 1 - grp
        landed = cross_wide.at[way, n % 2] if n < wide_cuts else cross_down.at[n - wide_cuts]
        return send(piece_of(n, 2, g), piece_of(n, 3, g), cross_send, landed, mate)

    def forward_again(n):
        arrived(piece_of(n, 2, 1 - grp), y_recv.at[n])
        cross_of(1, n).start()

    units = hid.shape[1] // 4

    depth = deep // 2

    def rows_of(a, b):
        return slice(a * capacity, b * capacity)

    def activate(gate, up, s, rows):
        hid[rows, s * units : (s + 1) * units] = (gate / (1.0 + jnp.exp(-gate)) * up).astype(BF16)

    def hidden(s, a, b):
        flat = rows_in[a:b].reshape((b - a) * capacity, deep)
        gate = jnp.dot(flat, g_all[s].reshape(deep, units), preferred_element_type=F32)
        up = jnp.dot(flat, u_all[s].reshape(deep, units), preferred_element_type=F32)
        activate(gate, up, s, rows_of(a, b))

    def hidden_near(s):
        hidden(s, 0, 2)

    def hidden_first_slot(s):
        hidden(s, 2, 3)

    def hidden_late(s):
        hidden(s, 3, 4)

    def half_of(s, g):
        cols = pl.ds(pl.multiple_of(g * depth, depth), depth)
        flat = rows_in[0:3, :, cols].reshape(3 * capacity, depth)
        gate = jnp.dot(flat, g_all[s, g].reshape(depth, units), preferred_element_type=F32)
        up = jnp.dot(flat, u_all[s, g].reshape(depth, units), preferred_element_type=F32)
        return gate, up

    def hidden_first(s):
        gate, up = half_of(s, grp)
        sofar[s - 2, 0] = gate
        sofar[s - 2, 1] = up

    def hidden_second(s):
        gate, up = half_of(s, 1 - grp)
        activate(sofar[s - 2, 0] + gate, sofar[s - 2, 1] + up, s, rows_of(0, 3))

    block = (span, span)
    key_sub = lax.broadcasted_iota(jnp.int32, block, 0)
    key_lane = lax.broadcasted_iota(jnp.int32, block, 1)
    after = (key_sub > key_lane).astype(BF16)
    past = key_lane < key_sub

    def attend(i, heads_now):
        for h in heads_now:
            cols = slice(h * head, (h + 1) * head)
            query = qkv_all[i, 0][:, cols] * BF16(head**-0.5)
            for j in range(i, -1, -1):
                z = lax.dot_general(
                    query,
                    qkv_all[j, 1][:, cols],
                    (((1,), (1,)), ((), ())),
                    preferred_element_type=F32,
                )
                z = z + bias_rows[j, pl.ds(me * heads + h, 1), :]
                stop = jnp.minimum(z, 0.0) - jnp.log(1.0 + jnp.exp(jnp.minimum(z, -z)))
                rest = stop - z
                if j == i:
                    rest = jnp.where(past, rest, 0.0)
                hi = rest.astype(BF16)
                left = rest - hi.astype(F32)
                mid = left.astype(BF16)
                low = (left - mid.astype(F32)).astype(BF16)
                sums = jnp.dot(
                    jnp.concatenate([hi, mid, low], axis=0), after, preferred_element_type=F32
                )
                within = sums[:span] + sums[span : 2 * span] + sums[2 * span :]
                local = jnp.exp(stop + within)
                if j == i:
                    local = jnp.where(past, local, 0.0)
                part = jnp.dot(
                    local.astype(BF16), qkv_all[j, 2][:, cols], preferred_element_type=F32
                )
                total = part if j == i else total + jnp.exp(carry) * part
                if j > 0:
                    tally = jnp.sum(rest, axis=1, keepdims=True)
                    carry = tally if j == i else carry + tally
            att_send[i, :, cols] = total.astype(BF16)
        if heads_now[-1] != heads - 1:
            return

        @pl.when(me == i)
        def _():
            att_all[i] = att_send[i]

        @pl.when(me != i)
        def _():
            att_of(i, me).start()

    def att_of(i, j):
        return send(att_send.at[i], att_all.at[j], att_ssem, att_rsem.at[j], {"ep": i})

    def packs_here():
        for copy in mine:
            copy.wait()
        loads[8].wait()
        for r in range(1, ep):
            source = lax.rem(me + r, ep)
            arrived(qkv_all.at[source], pack_recv.at[source])
            arrived(bias_all.at[source], bias_recv.at[source])
        bias_rows[...] = bias_all[...].astype(F32)

    firsts, lasts = tuple(range(heads // 2)), tuple(range(heads // 2, heads))
    everyone = firsts + lasts
    W = wide_cuts
    lag = 3
    near_at = (2, 4, 10)
    for n in range(W):
        forward(n)
        if n >= lag:
            forward_again(n - lag)
        if n in (7, 9, 11, 13):
            relay(0, (n - 7) // 2)
        if n in near_at:
            nears[near_at.index(n)].start()
        if n == 5:
            packs_here()
            attend(3, firsts)
        if n == 6:
            attend(3, lasts)
        if n == 7:
            attend(0, everyone)
        if n == 8:
            attend(2, everyone)
        if n == 9:
            attend(1, everyone)
        if n == 10:
            take(0)
            take(1)
        if n == 12:
            take(2)
        if n == 14:
            take(3)

            @pl.when(outside)
            def _():
                side_rows.wait_recv()

            hidden_near(0)
        if n == 15:
            for copy in nears:
                copy.wait_recv()
            hidden_near(1)

    forward_again(W - 3)
    forward(W)
    forward(W + 1)

    @pl.when(outside)
    def _():
        arrived(relay_out.at[0], relay_recv.at[0])

    hidden_first_slot(0)
    forward_again(W - 2)
    hidden_first_slot(1)
    relay(1, 0)
    forward(W + 2)
    for n, r in enumerate((g_all, u_all)):
        arrived(r.at[3, grp], cross_wide.at[0, n])
    hidden_first(2)
    hidden_first(3)
    forward(W + 3)
    forward_again(W - 1)
    hidden_second(2)
    forward_again(W)
    relay(1, 1)
    for n, r in enumerate((g_all, u_all)):
        arrived(r.at[3, 1 - grp], cross_wide.at[1, n])
    hidden_second(3)
    forward_again(W + 1)

    def outer_of(slot, c):
        cols = strip(c)
        return send(
            outer_out.at[slot, :, cols],
            outer_in.at[slot, :, cols],
            outer_send,
            outer_recv.at[slot, c],
            {"ep": side},
        )

    thirds = [
        slice(strip(a).start, strip(b).stop) for a, b in ((0, 3), (4, fine - 3), (fine - 2, fine - 1))
    ]

    def back_of(cols):
        return send(
            back_out.at[:, cols],
            back_in.at[1, :, cols],
            back_ssem,
            back_rsem.at[sum(cols.start >= e.start for e in thirds[1:])],
            {"ep": side},
        )

    def lower(cols, a, b):
        down = jnp.concatenate(
            [d_all[s, :, :, cols].reshape(units, -1) for s in range(4)], axis=0
        )
        return jnp.dot(hid[rows_of(a, b)], down, preferred_element_type=F32).astype(BF16)

    def put_far(slot, c, rows):
        outer_out[slot, :, strip(c)] = rows

        @pl.when(outside)
        def _():
            outer_of(slot, c).start()

    held = 3

    def final(c):
        cols = strip(c)
        arrived(d_all.at[3, :, :, cols], cross_down.at[c])
        rows = lower(cols, 0, 3)
        put_far(0, c, rows[rows_of(2, 3)])
        back_in[0, :, cols] = rows[rows_of(0, 1)]
        back_out[:, cols] = rows[rows_of(1, 2)]

        if c > held:

            @pl.when(inner)
            def _():
                back_of(cols).start()

    def final_late(c):
        put_far(1, c, lower(strip(c), 3, 4))

    def back_strips(first, last):
        @pl.when(outside)
        def _():
            back_of(slice(strip(first).start, strip(last).stop)).start()

    def home_of(slot, c):
        return send(
            dense_out.at[slot, :, strip(c)],
            dense_back.at[:, strip(c)],
            home_send,
            home_recv.at[c // (fine - 1)],
            {"ep": far[slot]},
        )

    def weigh(at, near_rows, far_rows):
        gate = gate_cols[at]
        here = jnp.dot(sel_back[2 * at], near_rows, preferred_element_type=F32)
        there = jnp.dot(sel_back[2 * at + 1], far_rows, preferred_element_type=F32)
        return gate[:, 0:1] * here + gate[:, 1:2] * there

    def return_home(slot, c):
        cols = strip(c)

        @pl.when(inner)
        def _():
            outer_of(slot, c).wait_recv()
            dense_out[slot, :, cols] = weigh(
                1 + slot, outer_out[slot, :, cols], outer_in[slot, :, cols]
            ).astype(BF16)
            home_of(slot, c).start()

    final(0)
    forward(W + 4)
    final(1)
    forward(W + 5)
    forward_again(W + 2)
    forward(W + 6)
    forward_again(W + 3)
    relay(1, 2)
    final(2)
    return_home(0, 0)
    relay(1, 3)
    return_home(0, 1)
    forward(W + 7)
    forward_again(W + 4)
    final(3)
    return_home(0, 2)

    @pl.when(inner)
    def _():
        back_of(slice(0, strip(held).stop)).start()

    forward(W + 8)
    forward_again(W + 5)
    final(4)
    back_strips(0, 1)
    return_home(0, 3)
    forward_again(W + 6)
    final(5)
    return_home(0, 4)
    forward_again(W + 7)
    final(6)
    return_home(0, 5)

    @pl.when(outside)
    def _():
        arrived(relay_out.at[1], relay_recv.at[1])

    hidden_late(0)
    hidden_late(1)
    forward_again(W + 8)
    final(7)
    return_home(0, 6)
    hidden_late(2)
    hidden_late(3)
    final(8)
    return_home(0, 7)
    return_home(0, 8)
    final_late(0)
    final_late(1)
    final_late(2)
    final_late(3)
    return_home(1, 0)
    return_home(1, 1)
    for c in range(4, fine):
        final_late(c)
    back_strips(2, 3)
    back_strips(4, fine - 3)
    back_strips(fine - 2, fine - 1)
    return_home(1, 2)
    for j in range(ep):

        @pl.when(me != j)
        def _():
            arrived(att_all.at[j], att_rsem.at[j])

    ow_copy.wait()
    attended = jnp.concatenate([att_all[j] for j in range(ep)], axis=1)
    term = jnp.dot(attended, ow[...], preferred_element_type=F32).astype(BF16)
    proj[...] = term.reshape(proj.shape)
    shares = [
        send(proj.at[mates[m]], proj_in.at[m], proj_ssem.at[m], proj_rsem.at[m], {"tp": mates[m]})
        for m in (2, 3, 1)
    ]
    for copy in shares:
        copy.start()
    for c in range(3, fine):
        return_home(1, c)
    whole = proj[tp].astype(F32)
    for copy in shares:
        copy.wait_recv()
    for m in (1, 2, 3):
        whole = whole + proj_in[m].astype(F32)
    loads[7].wait()
    scale = lax.rsqrt(jnp.mean(whole * whole, axis=-1, keepdims=True) + 1e-06)
    mixed_ref[...] = (whole * scale * mix_own[...]).astype(BF16)
    drained(normed_ref, dense_send)
    drained(g_all.at[pl.ds(0, 3), 0], x_send)
    drained(g_all.at[pl.ds(0, 3), 0], y_send)
    drained(g_all.at[pl.ds(0, 3)], cross_send)
    drained(g_all.at[pl.ds(0, 3)], near_send)
    drained(qkv_all.at[pl.ds(0, 3)], pack_send)
    drained(bias_all.at[pl.ds(0, ep - 1)], bias_send)

    @pl.when(inner)
    def _():
        side_rows.wait_send()
        drained(beside, pass_send)

    @pl.when(outside)
    def _():
        beside_table.wait_send()

    drained(meta, meta_send)
    drained(att_send.at[pl.ds(0, ep - 1)], att_ssem)

    for copy in shares:
        copy.wait_send()
    for n, cols in enumerate(thirds):
        arrived(back_in.at[1, :, cols], back_rsem.at[n])
        acc[:, cols] = weigh(0, back_in[0, :, cols], back_in[1, :, cols])
    drained(back_out, back_ssem)

    @pl.when(outside)
    def _():
        drained(outer_out, outer_send)

    for n, cols in enumerate((slice(0, strip(fine - 1).start), strip(fine - 1))):
        arrived(dense_back.at[:, cols], home_recv.at[n])
        out_ref[:, cols] = (acc[:, cols] + dense_back[:, cols].astype(F32)).astype(BF16)

    @pl.when(inner)
    def _():
        drained(relay_out, relay_send)
        drained(dense_out, home_send)


def settle_kernel(mixed_ref, out_ref, mixed_to, out_to, sems):
    copies = [
        pltpu.make_async_copy(out_ref, out_to, sems.at[0]),
        pltpu.make_async_copy(mixed_ref, mixed_to, sems.at[1]),
    ]
    for copy in copies:
        copy.start()
    for copy in copies:
        copy.wait()


def fused_device(
    groups,
    ep,
    tp,
    queries,
    keys,
    values,
    stop_bias,
    out_weight,
    mix_gain,
    moe_input,
    ffn_gain,
    expert_ids,
    expert_scores,
    gate_weight,
    up_weight,
    down_weight,
):
    span, cols = queries.shape
    tokens, deep = moe_input.shape
    top = expert_ids.shape[1]
    capacity = 3 * tokens * top // (2 * ep)
    width = cols // ep
    heads = stop_bias.shape[1]
    units = gate_weight.shape[2]
    cuts = 8
    parts = 4
    fine = 9
    lines = 8
    gate = gate_weight.reshape(groups, cuts, deep // (groups * cuts), units)
    up = up_weight.reshape(gate.shape)
    down = down_weight.reshape(groups, units // groups, deep)
    chunks = 2 * cuts + fine
    vmem = pl.BlockSpec(memory_space=pltpu.VMEM)
    hbm = pl.BlockSpec(memory_space=pl.ANY)
    dma = pltpu.SemaphoreType.DMA
    results = pl.pallas_call(
        functools.partial(layer_kernel, ep, capacity, cols // heads),
        out_shape=(
            pltpu.VMEM((span // tp, deep), BF16),
            pltpu.VMEM((tokens, deep), BF16),
        ),
        in_specs=[hbm] * 13,
        out_specs=(vmem, vmem),
        scratch_shapes=[
            pltpu.VMEM((tokens, deep), BF16),
            pltpu.VMEM((1, deep), F32),
            pltpu.VMEM((1, deep), F32),
            pltpu.VMEM((top, tokens), jnp.int32),
            pltpu.VMEM((top, tokens), F32),
            pltpu.VMEM((ep, 3, span, width), BF16),
            pltpu.VMEM((ep, heads, span), BF16),
            pltpu.VMEM((ep, heads, span), F32),
            pltpu.VMEM((ep, span, width), BF16),
            pltpu.VMEM((ep, span, width), BF16),
            pltpu.VMEM((tp, span // tp, deep), BF16),
            pltpu.VMEM((tp, span // tp, deep), BF16),
            pltpu.VMEM(out_weight.shape, BF16),
            pltpu.VMEM((lines, tokens), F32),
            pltpu.VMEM((2, lines, tokens), F32),
            pltpu.VMEM((tokens, deep), BF16),
            pltpu.VMEM((2, tokens, deep), BF16),
            pltpu.VMEM((tokens, deep), BF16),
            pltpu.VMEM((lines, tokens), F32),
            pltpu.VMEM((4, 2 * capacity, tokens), BF16),
            pltpu.VMEM((8, tokens, capacity), BF16),
            pltpu.VMEM((4, tokens, tokens), F32),
            pltpu.VMEM((capacity, deep), BF16),
            pltpu.VMEM((2, capacity, deep), BF16),
            pltpu.VMEM((ep, capacity, deep), BF16),
            pltpu.VMEM((ep * capacity, tp * units), BF16),
            pltpu.VMEM((2, 2, 3 * capacity, units), F32),
            pltpu.VMEM((tokens, deep), F32),
            pltpu.VMEM((capacity, deep), BF16),
            pltpu.VMEM((2, capacity, deep), BF16),
            pltpu.VMEM((2, capacity, deep), BF16),
            pltpu.VMEM((2, capacity, deep), BF16),
            pltpu.VMEM((2, tokens, deep), BF16),
            pltpu.VMEM((tokens, deep), BF16),
            pltpu.VMEM((4,) + gate.shape, BF16),
            pltpu.VMEM((4,) + up.shape, BF16),
            pltpu.VMEM((4,) + down.shape, BF16),
            dma((9,)),
            dma((3,)),
            dma(()),
            dma(()),
            dma((ep,)),
            dma(()),
            dma((ep,)),
            dma(()),
            dma(()),
            dma(()),
            dma((2,)),
            dma(()),
            dma((2, parts)),
            dma(()),
            dma((parts,)),
            dma(()),
            dma(()),
            dma(()),
            dma((2,)),
            dma(()),
            dma((ep,)),
            dma(()),
            dma((3,)),
            dma(()),
            dma((2, fine)),
            dma(()),
            dma((2,)),
            dma((tp,)),
            dma((tp,)),
            dma(()),
            dma((3,)),
            dma(()),
            dma((chunks,)),
            dma(()),
            dma((chunks,)),
            dma(()),
            dma((2, 2)),
            dma((fine,)),
        ],
        compiler_params=pltpu.CompilerParams(
            collective_id=0, has_side_effects=True, vmem_limit_bytes=60 * 2**20
        ),
    )(
        queries,
        keys,
        values,
        stop_bias.T,
        out_weight,
        mix_gain.reshape(1, deep),
        moe_input,
        ffn_gain.reshape(1, deep),
        expert_ids.T,
        expert_scores.T,
        gate,
        up,
        down,
    )
    results = [pltpu.with_memory_space_constraint(r, pltpu.VMEM) for r in results]
    return pl.pallas_call(
        settle_kernel,
        out_shape=tuple(jax.ShapeDtypeStruct(r.shape, r.dtype) for r in results),
        in_specs=[vmem] * 2,
        out_specs=(hbm, hbm),
        scratch_shapes=[dma((2,))],
    )(*results)


def pick_plan(groups, ep, tp, *args):
    heads = args[3].shape[1]
    width = args[0].shape[1] // ep
    head = args[0].shape[1] // heads
    exact = head & (head - 1) == 0 and head.bit_length() % 2 == 1
    if groups == 2 and tp == 4 and ep == 4 and heads % ep == 0 and width % 128 == 0 and exact:
        return fused_device(groups, ep, tp, *args)
    return per_device(*args)


def solution(mesh):
    return jax.shard_map(
        functools.partial(pick_plan, mesh.shape["grp"], mesh.shape["ep"], mesh.shape["tp"]),
        mesh=mesh,
        in_specs=(
            P(("grp", "ep"), "tp"),
            P(("grp", "ep"), "tp"),
            P(("grp", "ep"), "tp"),
            P(("grp", "ep"), "tp"),
            P("tp", None),
            P(),
            P(("grp", "ep", "tp"), None),
            P(),
            P(("grp", "ep", "tp"), None),
            P(("grp", "ep", "tp"), None),
            P("ep", None, "tp"),
            P("ep", None, "tp"),
            P("ep", "tp", None),
        ),
        out_specs=(P(("grp", "ep", "tp"), None), P(("grp", "ep", "tp"), None)),
        check_vma=False,
    )
```
